32 devices in a mesh: sp: 4 (over z), tp: 4 (over y, x), dp: 2 (over core).
Axes of the slice: x: 2, y: 2, z: 4, core: 2. Of those that a mesh axis runs over, the one named last changes fastest.
Arguments:
- latent: bfloat16 [4, 4096, 2048], P('dp', 'sp'), may hold values from -6 to 6
- context: bfloat16 [4, 1024, 2048], P('dp', 'sp'), may hold values from -6 to 6
- condition: bfloat16 [4, 2048], P('dp', 'sp'), may hold values from -6 to 6
- ctx_cond: bfloat16 [2048], P('sp'), may hold values from -6 to 6
- norm_gain: float32 [2048], replicated, may hold values from 0.1 to 1.9
- w_shift: bfloat16 [2048, 2048], P('sp', 'tp'), may hold values from -0.125 to 0.125
- w_scale: bfloat16 [2048, 2048], P('sp', 'tp'), may hold values from -0.125 to 0.125
- w_gate: bfloat16 [2048, 2048], P('sp', 'tp'), may hold values from -0.125 to 0.125
- w_query: bfloat16 [2048, 1024], P(None, 'tp'), may hold values from -0.125 to 0.125
- w_key: bfloat16 [2048, 256], P(None, 'tp'), may hold values from -0.125 to 0.125
- w_value: bfloat16 [2048, 256], P(None, 'tp'), may hold values from -0.125 to 0.125
- w_out: bfloat16 [1024, 2048], P('tp'), may hold values from -4 to 4
- sink_logit: float32 [16], P('tp'), may hold values from 4 to 7
- ctx_lift: float32 [16], P('tp'), may hold values from -4 to 220
Outputs:
- mixed: bfloat16 [4, 4096, 2048], P('dp', ('sp', 'tp'))
The draws below stay inside these ranges and needn't reach their ends.
All inputs are finite; a program needn't handle non-finite values.
Results may differ from the reference program's by a relative error of at most 0.012.
Values may be sent and summed in bfloat16 or wider, within the bound.
A program may use at most 128 MiB of HBM per device.

```python
import jax
import jax.numpy as jnp
from jax import lax

D = 2048
HEADS = 16
KV_HEADS = 4
HEAD = 64
WINDOW = 128
GRID_COLS = 64
TOK_DEV = 1024
CTX = 1024
SAMPLES = 4
LATENT = 4096


def draw_ctx_lift(key, part):
    first_key = jax.random.fold_in(key, 11)
    lifted = jax.random.uniform(first_key, (HEADS,), jnp.float32, -3.6, -1.8)
    return lifted


def level_of(own_key, dims, cuts, smallest, largest):
    factor_of = 1.0
    for position, blocks in cuts:
        steps = jax.random.uniform(jax.random.fold_in(jax.random.fold_in(own_key, 6), position), (blocks,), jnp.float32, smallest / len(cuts), largest / len(cuts))
        factor_of = factor_of * jnp.repeat(jnp.exp(steps), dims[position] // blocks).reshape((-1,) + (1,) * (len(dims) - 1 - position))
    return factor_of


def centred(stream_key, shape, deviation, limit, cuts=(), kind=jnp.bfloat16):
    level = level_of(stream_key, shape, cuts, -0.22, 0.18) if cuts else 1.0
    array = jax.random.normal(stream_key, shape, jnp.float32) * deviation * level
    return jnp.minimum(jnp.maximum(array, -limit), limit).astype(kind)


def setup_inputs(seed: int = 0) -> dict:
    splits = jax.random.split(jax.random.key(seed), 15)
    return {
        "latent": centred(splits[0], (SAMPLES, LATENT, D), 1.0, 6.0, ((0, 2), (1, 4))),
        "context": centred(splits[1], (SAMPLES, CTX, D), 1.0, 6.0, ((0, 2), (1, 4))),
        "condition": centred(splits[2], (SAMPLES, D), 1.0, 6.0, ((0, 2), (1, 4))),
        "ctx_cond": centred(splits[3], (D,), 1.0, 6.0, ((0, 4),)),
        "norm_gain": jnp.clip(1.0 + 0.18 * jax.random.normal(splits[4], (D,), jnp.float32), 0.1, 1.9),
        "w_shift": centred(splits[5], (D, D), D ** -0.5, 0.125, ((0, 4), (1, 4))),
        "w_scale": centred(splits[6], (D, D), D ** -0.5, 0.125, ((0, 4), (1, 4))),
        "w_gate": centred(splits[7], (D, D), D ** -0.5, 0.125, ((0, 4), (1, 4))),
        "w_query": centred(splits[8], (D, HEADS * HEAD), D ** -0.5, 0.125, ((1, 4),)),
        "w_key": centred(splits[9], (D, KV_HEADS * HEAD), D ** -0.5, 0.125, ((1, 4),)),
        "w_value": centred(splits[10], (D, KV_HEADS * HEAD), D ** -0.5, 0.125, ((1, 4),)),
        "w_out": centred(splits[11], (HEADS * HEAD, D), 2 ** -0.5, 4.0, ((0, 4),)),
        "sink_logit": jnp.clip(4.0 + 3.0 * jax.random.uniform(splits[12], (HEADS,), jnp.float32) ** level_of(splits[12], (HEADS,), ((0, 4),), -0.2, 0.2), 4.0, 7.0),
        "ctx_lift": draw_ctx_lift(jax.random.fold_in(splits[14], 71), 0),
    }


epsilon = 1e-06
rope_base = 10000.0
masked_value = -1e+30

def modulated(inputs, norm_gain, shift_vec, scale_vec):
    widened = inputs.astype(jnp.float32)
    inverse = lax.rsqrt(lax.optimization_barrier(jnp.mean(widened * widened, axis=-1, keepdims=True)) + epsilon)
    return (widened * inverse * norm_gain * (1.0 + scale_vec) + shift_vec).astype(jnp.bfloat16)

def rotate_half(half_part, angles):
    first_half, second = jnp.split(half_part, 2, axis=-1)
    cosine = jnp.cos(angles)[:, None, :]
    sine_part = jnp.sin(angles)[:, None, :]
    return jnp.concatenate([first_half * cosine - second * sine_part, first_half * sine_part + second * cosine], axis=-1)

def rotate(inputs, positions):
    quarter = inputs.shape[-1] // 4
    frequency = rope_base ** (-jnp.arange(quarter, dtype=jnp.float32) / quarter)
    row_angle = (positions // GRID_COLS).astype(jnp.float32)[:, None] * frequency
    col_angle = (positions % GRID_COLS).astype(jnp.float32)[:, None] * frequency
    half_size = 2 * quarter
    return jnp.concatenate([rotate_half(inputs[..., :half_size], row_angle), rotate_half(inputs[..., half_size:], col_angle)], axis=-1)

def reference(latent, context, condition, ctx_cond, norm_gain, w_shift, w_scale, w_gate, w_query, w_key, w_value, w_out, sink_logit, ctx_lift):
    samples, latent_len, model_width = latent.shape
    cond_rows = jnp.concatenate([condition, ctx_cond[None, :]], axis=0)
    active = jax.nn.silu(cond_rows.astype(jnp.float32)).astype(jnp.bfloat16)
    shift_vec = jnp.dot(active, w_shift, preferred_element_type=jnp.float32)
    scale_vec = jnp.dot(active, w_scale, preferred_element_type=jnp.float32)
    gate_vec = jnp.dot(active, w_gate, preferred_element_type=jnp.float32)
    hidden = modulated(latent, norm_gain, shift_vec[:samples, None, :], scale_vec[:samples, None, :])
    ctx_hidden = modulated(context, norm_gain, shift_vec[samples], scale_vec[samples])
    positions = jnp.arange(latent_len, dtype=jnp.int32)
    flat = hidden.reshape(-1, model_width)
    queries = rotate(jnp.dot(flat, w_query, preferred_element_type=jnp.float32).reshape(samples, latent_len, HEADS, HEAD), positions).astype(jnp.bfloat16)
    key_rows = rotate(jnp.dot(flat, w_key, preferred_element_type=jnp.float32).reshape(samples, latent_len, KV_HEADS, HEAD), positions).astype(jnp.bfloat16)
    values = jnp.dot(flat, w_value, preferred_element_type=jnp.float32).astype(jnp.bfloat16).reshape(samples, latent_len, KV_HEADS, HEAD)
    ctx_flat = ctx_hidden.reshape(-1, model_width)
    ctx_keys = jnp.dot(ctx_flat, w_key, preferred_element_type=jnp.float32).astype(jnp.bfloat16).reshape(samples, CTX, KV_HEADS, HEAD)
    ctx_values = jnp.dot(ctx_flat, w_value, preferred_element_type=jnp.float32).astype(jnp.bfloat16).reshape(samples, CTX, KV_HEADS, HEAD)
    padding = ((0, 0), (WINDOW, WINDOW), (0, 0), (0, 0))
    key_pad = jnp.pad(key_rows, padding)
    value_pad = jnp.pad(values, padding)
    block_rows = min(512, TOK_DEV)
    blocks = latent_len // block_rows
    span_rows = block_rows + 2 * WINDOW
    group_size = HEADS // KV_HEADS
    lift_rows = ctx_lift.astype(jnp.float32).reshape(KV_HEADS, group_size, 1, 1)
    sink_rows = sink_logit.astype(jnp.float32).reshape(KV_HEADS, group_size, 1, 1)
    factor = HEAD ** (-0.5)

    def attend(step_id):
        sample = step_id // blocks
        row_start = step_id % blocks * block_rows
        q_rows = lax.dynamic_slice_in_dim(lax.dynamic_index_in_dim(queries, sample, 0, keepdims=False), row_start, block_rows, 0)
        q_rows = q_rows.reshape(block_rows, KV_HEADS, group_size, HEAD).astype(jnp.float32)
        near_keys = lax.dynamic_slice_in_dim(lax.dynamic_index_in_dim(key_pad, sample, 0, keepdims=False), row_start, span_rows, 0).astype(jnp.float32)
        near_values = lax.dynamic_slice_in_dim(lax.dynamic_index_in_dim(value_pad, sample, 0, keepdims=False), row_start, span_rows, 0).astype(jnp.float32)
        far_keys = lax.dynamic_index_in_dim(ctx_keys, sample, 0, keepdims=False).astype(jnp.float32)
        far_values = lax.dynamic_index_in_dim(ctx_values, sample, 0, keepdims=False).astype(jnp.float32)
        query_pos = row_start + jnp.arange(block_rows, dtype=jnp.int32)
        key_pos = row_start - WINDOW + jnp.arange(span_rows, dtype=jnp.int32)
        inside = (key_pos[None, :] >= 0) & (key_pos[None, :] < latent_len) & (jnp.abs(query_pos[:, None] - key_pos[None, :]) <= WINDOW)
        near_scores = jnp.einsum('qgrd,kgd->grqk', q_rows, near_keys) * factor
        near_scores = jnp.where(inside[None, None], near_scores, masked_value)
        far_scores = jnp.einsum('qgrd,kgd->grqk', q_rows, far_keys) * factor + lift_rows
        row_max = jnp.maximum(jnp.maximum(near_scores.max(-1, keepdims=True), far_scores.max(-1, keepdims=True)), sink_rows)
        near_exp = jnp.exp(near_scores - row_max)
        far_exp = jnp.exp(far_scores - row_max)
        normaliser = near_exp.sum(-1, keepdims=True) + far_exp.sum(-1, keepdims=True) + jnp.exp(sink_rows - row_max)
        near_weights = (near_exp / normaliser).astype(jnp.bfloat16).astype(jnp.float32)
        far_weights = (far_exp / normaliser).astype(jnp.bfloat16).astype(jnp.float32)
        outcome = jnp.einsum('grqk,kgd->qgrd', near_weights, near_values) + jnp.einsum('grqk,kgd->qgrd', far_weights, far_values)
        return outcome.astype(jnp.bfloat16).reshape(block_rows, HEADS * HEAD)
    attended = lax.map(attend, jnp.arange(samples * blocks, dtype=jnp.int32)).reshape(samples, latent_len, HEADS * HEAD)
    projected = jnp.dot(attended.reshape(-1, HEADS * HEAD), w_out, preferred_element_type=jnp.float32).reshape(samples, latent_len, model_width)
    return (gate_vec[:samples, None, :] * projected).astype(jnp.bfloat16)
```

```python
import functools
import math

import jax
import jax.numpy as jnp
from jax import lax
from jax.experimental import pallas as pl
from jax.experimental.pallas import tpu as pltpu
from jax.sharding import PartitionSpec as P

HEAD = 64
WINDOW = 128
GRID_COLS = 64
LANES = 128
ONES = 16

epsilon = 1e-06
rope_base = 10000.0
masked_value = -1e30
log2e = 1.4426950408889634
MESH = pl.DeviceIdType.MESH
nt = (((1,), (1,)), ((), ()))
f32 = jnp.float32
bf16 = jnp.bfloat16


def kernel(
    sizes,
    latent,
    context,
    condition,
    ctx_cond,
    norm_gain,
    w_shift,
    w_scale,
    w_gate,
    w_query,
    w_key,
    w_value,
    w_out,
    sink_logit,
    ctx_lift,
    out,
    x_lat,
    x_ctx,
    w_mod,
    w_q,
    w_t,
    w_s,
    w_c,
    cos_row,
    sin_row,
    cos_col,
    sin_col,
    w_o,
    act,
    mod_rx,
    mod_all,
    gate_rx,
    gate_all,
    vec_a,
    vec_b,
    vec_g,
    inv_lat,
    inv_ctx,
    bias_col,
    bias_row,
    q_buf,
    kv_buf,
    vt_buf,
    ckv_buf,
    cvt_buf,
    mask_buf,
    s_a,
    s_b,
    att_buf,
    rows_rx,
    ld_sem,
    ma_send,
    ma_recv,
    mb_send,
    mb_recv,
    ga_send,
    ga_recv,
    gb_send,
    gb_recv,
    cx_send,
    cx_recv,
    ha_send,
    ha_recv,
    at_send,
    at_recv,
    wo_send,
    wo_recv,
    wf_send,
    wf_recv,
):
    n_sp, n_tp, n_dp = sizes
    me_sp, me_tp, me_dp = lax.axis_index("sp"), lax.axis_index("tp"), lax.axis_index("dp")
    samples, tokens, width = latent.shape
    ctx_rows = context.shape[1]
    ctx_all = n_sp * ctx_rows
    part = w_shift.shape[1]
    q_cols = w_query.shape[1]
    heads = q_cols // HEAD
    block = tokens // n_tp
    quarter = HEAD // 4
    q_scale = log2e * HEAD ** (-0.5)

    def other(me, step, count):
        return lax.rem(me + step, count)

    barrier = pltpu.get_barrier_semaphore()
    for axis, me, count in (("sp", me_sp, n_sp), ("tp", me_tp, n_tp), ("dp", me_dp, n_dp)):
        for step in range(1, count):
            pl.semaphore_signal(
                barrier, inc=1, device_id={axis: other(me, step, count)}, device_id_type=MESH
            )

    loads = []
    for source, target in (
        (w_shift, w_mod.at[0]),
        (w_scale, w_mod.at[1]),
        (context, x_ctx),
        (w_key, w_t.at[q_cols : q_cols + HEAD]),
        (w_value, w_t.at[q_cols + HEAD : q_cols + 2 * HEAD]),
        (w_query, w_q),
        (w_gate, w_mod.at[2]),
        *((latent.at[s], x_lat.at[s]) for s in range(samples)),
        (w_out, w_o.at[me_tp]),
    ):
        copy = pltpu.make_async_copy(source, target, ld_sem.at[len(loads)])
        copy.start()
        loads.append(copy)

    def peers(axis, me, count, buffer, send, recv):
        def copy(step, source):
            return pltpu.make_async_remote_copy(
                src_ref=buffer.at[source],
                dst_ref=buffer.at[source],
                send_sem=send.at[step],
                recv_sem=recv.at[step],
                device_id={axis: other(me, step, count)},
                device_id_type=MESH,
            )

        def start():
            for step in range(1, count):
                copy(step, me).start()

        def arrive():
            for step in range(1, count):
                copy(step, other(me, count - step, count)).wait_recv()

        def finish():
            for step in range(1, count):
                copy(step, me).wait_send()

        return start, arrive, finish

    mod_a = peers("sp", me_sp, n_sp, mod_rx, ma_send, ma_recv)
    mod_b = peers("tp", me_tp, n_tp, mod_all, mb_send, mb_recv)
    gate_a = peers("sp", me_sp, n_sp, gate_rx, ga_send, ga_recv)
    gate_b = peers("tp", me_tp, n_tp, gate_all, gb_send, gb_recv)
    keep_rows = mod_rx.shape[1]

    act[...] = jnp.zeros_like(act)
    cond = condition[...].astype(f32)
    act[0:samples, :] = cond / (1.0 + jnp.exp(-cond))
    cond = ctx_cond[...].astype(f32).reshape(1, -1)
    act[samples : samples + 1, :] = cond / (1.0 + jnp.exp(-cond))
    active = act[...].astype(bf16)
    for i in range(2):
        loads[i].wait()
        mod_rx[me_sp, :, i * part : (i + 1) * part] = jnp.dot(
            active, w_mod[i], preferred_element_type=f32
        )[0:keep_rows]
    pl.semaphore_wait(barrier, n_sp + n_tp + n_dp - 3)
    mod_a[0]()

    loads[6].wait()
    gate_rx[me_sp] = jnp.dot(active, w_mod[2], preferred_element_type=f32)[0:keep_rows]
    gate_a[0]()

    loads[2].wait()
    for s in range(samples):
        wide = x_ctx[s].astype(f32)
        total = jnp.sum(wide * wide, axis=-1, keepdims=True)
        inv_ctx[s] = jnp.broadcast_to(lax.rsqrt(total / width + epsilon), (ctx_rows, LANES))

    loads[3].wait()
    loads[4].wait()
    loads[5].wait()
    for i in range(0, width, 256):
        w_t[0:q_cols, i : i + 256] = w_q[i : i + 256, :].T

    fill_tables(me_sp * (tokens // GRID_COLS), cos_row, sin_row, cos_col, sin_col)
    key_id = lax.broadcasted_iota(jnp.int32, (WINDOW, LANES), 0)
    query_id = lax.broadcasted_iota(jnp.int32, (WINDOW, LANES), 1)
    mask_buf[0] = jnp.where(key_id >= query_id, 0.0, masked_value)
    mask_buf[1] = jnp.where(key_id <= query_id, 0.0, masked_value)
    q_buf[:, :, HEAD:, :] = jnp.zeros(q_buf.shape[:2] + (LANES - HEAD, tokens), bf16)
    vt_buf[:, HEAD:, :] = jnp.ones((samples, ONES, vt_buf.shape[2]), bf16)
    cvt_buf[:, HEAD:, :] = jnp.ones((samples, ONES, ctx_all), bf16)
    vec_b[...] = jnp.zeros_like(vec_b)

    def stats(s):
        def body(i, carry):
            rows = pl.ds(pl.multiple_of(i * block, block), block)
            wide = x_lat[s, rows, :].astype(f32)
            acc = wide[:, 0:LANES] * wide[:, 0:LANES]
            for k in range(LANES, width, LANES):
                acc = acc + wide[:, k : k + LANES] * wide[:, k : k + LANES]
            total = jnp.sum(acc.T, axis=0, keepdims=True)
            inv_lat[s, :, rows] = lax.rsqrt(total / width + epsilon)
            return carry

        lax.fori_loop(0, n_tp, body, 0)

    loads[7].wait()
    stats(0)

    mod_a[1]()
    total = mod_rx[0]
    for i in range(1, n_sp):
        total = total + mod_rx[i]
    mod_all[me_tp] = total
    mod_b[0]()

    for s in range(1, samples):
        loads[7 + s].wait()
        stats(s)

    gate_a[1]()
    total = gate_rx[0]
    for i in range(1, n_sp):
        total = total + gate_rx[i]
    gate_all[me_tp] = total
    gate_b[0]()

    mod_b[1]()
    for t in range(n_tp):
        cols = slice(t * part, (t + 1) * part)
        vec_b[0:keep_rows, cols] = mod_all[t, :, 0:part]
        vec_a[0:keep_rows, cols] = (1.0 + mod_all[t, :, part : 2 * part]) * norm_gain[:, cols]

    share = w_out.shape[0] // n_dp
    mine = pl.ds(pl.multiple_of(me_dp * share, share), share)

    def out_copy(step, source):
        return pltpu.make_async_remote_copy(
            src_ref=w_out.at[mine, :],
            dst_ref=w_o.at[source, mine, :],
            send_sem=wo_send.at[step],
            recv_sem=wo_recv.at[step],
            device_id={"tp": other(me_tp, step, n_tp)},
            device_id_type=MESH,
        )

    def forward_copy(step, hop, part_id):
        source = other(me_tp, n_tp - step, n_tp)
        rows = pl.ds(pl.multiple_of(part_id * share, share), share)
        return pltpu.make_async_remote_copy(
            src_ref=w_o.at[source, rows, :],
            dst_ref=w_o.at[source, rows, :],
            send_sem=wf_send.at[step, hop],
            recv_sem=wf_recv.at[step, hop],
            device_id={"dp": other(me_dp, hop, n_dp)},
            device_id_type=MESH,
        )

    for step in range(1, n_tp):
        out_copy(step, me_tp).start()

    def fold(target, first, last, base, row):
        gain = vec_a[row : row + 1, :]
        for r in range(first, last, 32):
            target[r - base : r - base + 32, :] = (w_t[r : r + 32, :].astype(f32) * gain).astype(bf16)

    shift = vec_b[...]
    high = shift.astype(bf16).astype(f32)
    shift_pair = jnp.concatenate([high, shift - high], axis=0).astype(bf16)
    bias = lax.dot_general(shift_pair, w_t[q_cols:, :], nt, preferred_element_type=f32)
    bias_row[...] = bias[0:8] + bias[8:16]
    fold(w_c, q_cols, q_cols + 2 * HEAD, q_cols, samples)

    def ctx_copy(s, step, source):
        rows = pl.ds(pl.multiple_of(source * ctx_rows, ctx_rows), ctx_rows)
        return pltpu.make_async_remote_copy(
            src_ref=ckv_buf.at[s, rows, :],
            dst_ref=ckv_buf.at[s, rows, :],
            send_sem=cx_send.at[s, step],
            recv_sem=cx_recv.at[s, step],
            device_id={"sp": other(me_sp, step, n_sp)},
            device_id_type=MESH,
        )

    for s in range(samples):
        rows = pl.ds(pl.multiple_of(me_sp * ctx_rows, ctx_rows), ctx_rows)
        kv = lax.dot_general(x_ctx[s], w_c[...], nt, preferred_element_type=f32)
        ckv_buf[s, rows, :] = (kv * inv_ctx[s] + bias_row[samples : samples + 1, :]).astype(bf16)
        for step in range(1, n_sp):
            ctx_copy(s, step, me_sp).start()

    bias = lax.dot_general(w_t[...], shift_pair, nt, preferred_element_type=f32)
    for s in range(samples):
        column = bias[:, s : s + 1] + bias[:, 8 + s : 9 + s]
        bias_col[s, 0:q_cols, :] = jnp.broadcast_to(column[0:q_cols] * q_scale, (q_cols, LANES))
        bias_col[s, q_cols:, :] = jnp.broadcast_to(column[q_cols:], (2 * HEAD, LANES))
        fold(w_s.at[s], 0, q_cols + 2 * HEAD, 0, s)

    def halo_copy(s, side):
        source, target = ((tokens, 0), (WINDOW, WINDOW + tokens))[side]
        step = (1, n_sp - 1)[side]
        return pltpu.make_async_remote_copy(
            src_ref=kv_buf.at[s, pl.ds(source, WINDOW), :],
            dst_ref=kv_buf.at[s, pl.ds(target, WINDOW), :],
            send_sem=ha_send.at[s, side],
            recv_sem=ha_recv.at[s, side],
            device_id={"sp": other(me_sp, step, n_sp)},
            device_id_type=MESH,
        )

    def project(s, start):
        cols = slice(start, start + block)
        y = lax.dot_general(w_s[s], x_lat[s, cols, :], nt, preferred_element_type=f32)
        inv = inv_lat[s, :, cols]
        inv_q = inv * q_scale
        cr, sr = cos_row[:, cols], sin_row[:, cols]
        cc, sc = cos_col[...], sin_col[...]

        def wide(first, count):
            return jnp.concatenate([bias_col[s, first : first + count, :]] * (block // LANES), axis=1)

        def rotated(base, scale):
            u = [
                y[base + k * quarter : base + (k + 1) * quarter] * scale
                + wide(base + k * quarter, quarter)
                for k in range(4)
            ]
            return (
                u[0] * cr - u[1] * sr,
                u[0] * sr + u[1] * cr,
                u[2] * cc - u[3] * sc,
                u[2] * sc + u[3] * cc,
            )

        for h in range(heads):
            q_buf[s, h, 0:HEAD, cols] = jnp.concatenate(rotated(h * HEAD, inv_q), axis=0).astype(bf16)
        v = y[q_cols + HEAD :] * inv + wide(q_cols + HEAD, HEAD)
        kv = jnp.concatenate((*rotated(q_cols, inv), v), axis=0)
        vt_buf[s, 0:HEAD, WINDOW + start : WINDOW + start + block] = v.astype(bf16)
        kv_buf[s, WINDOW + start : WINDOW + start + block, :] = kv.T.astype(bf16)

    for s in range(samples):
        for i in range(n_tp):
            project(s, i * block)
        halo_copy(s, 0).start()
        halo_copy(s, 1).start()

    def rows_copy(s, step, source):
        target = other(me_tp, step, n_tp)
        return pltpu.make_async_remote_copy(
            src_ref=att_buf.at[s, target],
            dst_ref=rows_rx.at[source, s],
            send_sem=at_send.at[s, step],
            recv_sem=at_recv.at[s, step],
            device_id={"tp": target},
            device_id_type=MESH,
        )

    pairs = heads // 2
    halves = block // LANES
    near_rows = LANES + 2 * WINDOW
    low = lax.broadcasted_iota(jnp.int32, (1, 2 * LANES), 1) < LANES

    def two(ref, pair):
        return jnp.where(low, ref[2 * pair], ref[2 * pair + 1]) * log2e

    def start_of(index):
        step = index // halves + 1
        owner = other(me_tp, step, n_tp)
        return pl.multiple_of(owner * block + (index % halves) * LANES, LANES)

    chunks = [(False, 0, 2 * WINDOW), (False, 2 * WINDOW, LANES)]
    far_chunk = min(256, ctx_all)
    for c in range(0, ctx_all, far_chunk):
        chunks.append((True, c, far_chunk))

    def score_steps(s, index, pair, buf, state):
        start = start_of(index)
        cols = pl.ds(start, LANES)
        q = jnp.concatenate(
            [q_buf[s, 2 * pair, :, cols], q_buf[s, 2 * pair + 1, :, cols]], axis=1
        )
        tops = [None, None]

        def one(chunk):
            far, first, count = chunk
            if far:
                keys = ckv_buf[s, first : first + count, :]
            else:
                keys = kv_buf[s, pl.ds(start + first, count), :]
            scores = jnp.dot(keys, q, preferred_element_type=f32)
            base = near_rows + first if far else first
            if not far:
                mask = mask_buf[0 if first == 0 else 1]
                mask = jnp.concatenate([mask, mask], axis=1)
                edge = scores[0:WINDOW] + mask
                if count > WINDOW:
                    scores = jnp.concatenate([edge, scores[WINDOW:]], axis=0)
                else:
                    scores = edge
            buf[base : base + count, :] = scores
            high = jnp.max(scores.reshape(count // 8, 8, 2 * LANES), axis=0)
            tops[far] = high if tops[far] is None else jnp.maximum(tops[far], high)

        for chunk in chunks:
            yield functools.partial(one, chunk)

        def close():
            near_top = jnp.max(tops[0], axis=0, keepdims=True)
            far_top = jnp.max(tops[1], axis=0, keepdims=True)
            lift = two(ctx_lift, pair)
            state.append(
                jnp.maximum(jnp.maximum(near_top, far_top + lift), two(sink_logit, pair))
            )

        yield close

    def value_steps(s, index, pair, buf, top):
        start = start_of(index)
        far_top = top - two(ctx_lift, pair)
        acc = [None]

        def one(chunk):
            far, first, count = chunk
            base = near_rows + first if far else first
            p = jnp.exp2(buf[base : base + count, :] - (far_top if far else top)).astype(bf16)
            if far:
                values = cvt_buf[s, :, first : first + count]
            else:
                values = vt_buf[s, :, pl.ds(start + first, count)]
            term = jnp.dot(values, p, preferred_element_type=f32)
            acc[0] = term if acc[0] is None else acc[0] + term

        for chunk in chunks:
            yield functools.partial(one, chunk)

        def close():
            weight = acc[0][HEAD : HEAD + 1] + jnp.exp2(two(sink_logit, pair) - top)
            rows = acc[0][0:HEAD] * (1.0 / weight)
            stacked = jnp.concatenate([rows[:, 0:LANES], rows[:, LANES:]], axis=0)
            owner = other(me_tp, index // halves + 1, n_tp)
            half = pl.multiple_of((index % halves) * LANES, LANES)
            att_buf[s, owner, pl.ds(half, LANES), pair * LANES : (pair + 1) * LANES] = (
                stacked.T.astype(bf16)
            )

        yield close

    def run(*streams):
        for steps in zip(*streams):
            for step in steps:
                step()

    bufs = (s_a, s_b)

    def attention(s):
        count = n_tp * halves
        top0 = []
        run(score_steps(s, 0, 0, s_a, top0))

        def body(index, top, last):
            for pair in range(pairs):
                mine_buf, next_buf = bufs[pair % 2], bufs[(pair + 1) % 2]
                fresh = []
                streams = [value_steps(s, index, pair, mine_buf, top)]
                if pair + 1 < pairs:
                    streams.insert(0, score_steps(s, index, pair + 1, next_buf, fresh))
                elif not last:
                    streams.insert(0, score_steps(s, index + 1, 0, next_buf, fresh))
                run(*streams)
                top = fresh[0] if fresh else top

            step = index // halves + 1

            @pl.when((index % halves == halves - 1) & (step < n_tp))
            def _():
                rows_copy(s, step, me_tp).start()

            return top

        top = lax.fori_loop(0, count - 1, lambda i, top: body(i, top, False), top0[0])
        body(count - 1, top, True)
        rows_rx[me_tp, s] = att_buf[s, me_tp]

    def context_ready(s):
        for step in range(1, n_sp):
            ctx_copy(s, step, other(me_sp, n_sp - step, n_sp)).wait_recv()
        for c in range(0, ctx_all, 256):
            cvt_buf[s, 0:HEAD, c : c + 256] = ckv_buf[s, c : c + 256, :].T[HEAD:]

    def halo_ready(s):
        for side in range(2):
            halo_copy(s, side).wait_recv()
            first = (0, WINDOW + tokens)[side]
            valid = (me_sp > 0, me_sp < n_sp - 1)[side]
            rows = jnp.where(valid, kv_buf[s, first : first + WINDOW, :].astype(f32), 0.0)
            kv_buf[s, first : first + WINDOW, :] = rows.astype(bf16)
            vt_buf[s, 0:HEAD, first : first + WINDOW] = rows.T[HEAD:].astype(bf16)
            vt_buf[s, HEAD:, first : first + WINDOW] = jnp.where(
                valid, jnp.ones((ONES, WINDOW), f32), 0.0
            ).astype(bf16)

    for s in range(samples):
        halo_ready(s)
        context_ready(s)
        attention(s)
        if s == 0:
            for step in range(1, n_tp):
                out_copy(step, other(me_tp, n_tp - step, n_tp)).wait_recv()
                for hop in range(1, n_dp):
                    forward_copy(step, hop, me_dp).start()

    gate_b[1]()
    for t in range(n_tp):
        vec_g[0:keep_rows, t * part : (t + 1) * part] = gate_all[t]

    loads[-1].wait()
    for step in range(1, n_tp):
        for hop in range(1, n_dp):
            forward_copy(step, hop, other(me_dp, n_dp - hop, n_dp)).wait_recv()
    chunk = 512
    for s in range(samples):
        for step in range(1, n_tp):
            rows_copy(s, step, other(me_tp, n_tp - step, n_tp)).wait_recv()

        def finish(i, carry):
            cols = pl.ds(pl.multiple_of(i * chunk, chunk), chunk)
            acc = jnp.dot(rows_rx[0, s], w_o[0, :, cols], preferred_element_type=f32)
            for t in range(1, n_tp):
                acc += jnp.dot(rows_rx[t, s], w_o[t, :, cols], preferred_element_type=f32)
            out[s, :, cols] = (acc * vec_g[s : s + 1, cols]).astype(bf16)
            return carry

        lax.fori_loop(0, width // chunk, finish, 0)

    for _, _, finish_send in (mod_a, mod_b, gate_a, gate_b):
        finish_send()
    for s in range(samples):
        for step in range(1, n_sp):
            ctx_copy(s, step, me_sp).wait_send()
        halo_copy(s, 0).wait_send()
        halo_copy(s, 1).wait_send()
    for step in range(1, n_tp):
        out_copy(step, me_tp).wait_send()
        for hop in range(1, n_dp):
            forward_copy(step, hop, me_dp).wait_send()
        for s in range(samples):
            rows_copy(s, step, me_tp).wait_send()


def fill_tables(first_row, cos_row, sin_row, cos_col, sin_col):
    tokens = cos_row.shape[1]
    quarter = HEAD // 4

    def pair(ticks, shape):
        power = lax.broadcasted_iota(jnp.int32, shape, 0).astype(f32)
        angles = ticks.astype(f32) * jnp.exp(power * (-math.log(rope_base) / quarter))
        return jnp.cos(angles), jnp.sin(angles)

    shape = cos_col.shape
    token = lax.broadcasted_iota(jnp.int32, shape, 1)
    cos_col[...], sin_col[...] = pair(token % GRID_COLS, shape)
    lines = tokens // GRID_COLS
    shape = (quarter, LANES)
    for first in range(0, lines, LANES):
        line = lax.broadcasted_iota(jnp.int32, shape, 1) + first + first_row
        cos_all, sin_all = pair(line, shape)
        half = lax.broadcasted_iota(jnp.int32, shape, 1) < GRID_COLS
        for r in range(0, min(LANES, lines - first), 2):
            cols = slice((first + r) * GRID_COLS, (first + r + 2) * GRID_COLS)
            for source, target in ((cos_all, cos_row), (sin_all, sin_row)):
                target[:, cols] = jnp.where(half, source[:, r : r + 1], source[:, r + 1 : r + 2])


def shards(
    latent,
    context,
    condition,
    ctx_cond,
    norm_gain,
    w_shift,
    w_scale,
    w_gate,
    w_query,
    w_key,
    w_value,
    w_out,
    sink_logit,
    ctx_lift,
):
    samples, tokens, width = latent.shape
    ctx_rows = context.shape[1]
    n_sp, n_tp, n_dp = lax.axis_size("sp"), lax.axis_size("tp"), lax.axis_size("dp")
    q_cols = w_query.shape[1]
    heads = q_cols // HEAD
    assert w_key.shape[1] == HEAD and tokens % GRID_COLS == 0 and samples < 4 and heads % 4 == 0
    part = w_shift.shape[1]
    block = tokens // n_tp
    ctx_all = n_sp * ctx_rows
    vmem = pl.BlockSpec(memory_space=pltpu.VMEM)
    smem = pl.BlockSpec(memory_space=pltpu.SMEM)
    anywhere = pl.BlockSpec(memory_space=pl.ANY)
    dma = pltpu.SemaphoreType.DMA
    padded = tokens + 2 * WINDOW
    proj = q_cols + 2 * HEAD
    keys = LANES + 2 * WINDOW + ctx_all
    V = pltpu.VMEM
    return pl.pallas_call(
        functools.partial(kernel, (n_sp, n_tp, n_dp)),
        out_shape=jax.ShapeDtypeStruct((samples, block, width), bf16),
        in_specs=[anywhere] * 2 + [vmem] * 3 + [anywhere] * 7 + [smem] * 2,
        out_specs=vmem,
        scratch_shapes=[
            V(latent.shape, bf16),
            V(context.shape, bf16),
            V((3,) + w_shift.shape, bf16),
            V(w_query.shape, bf16),
            V((proj, width), bf16),
            V((samples, proj, width), bf16),
            V((2 * HEAD, width), bf16),
            V((HEAD // 4, tokens), f32),
            V((HEAD // 4, tokens), f32),
            V((HEAD // 4, block), f32),
            V((HEAD // 4, block), f32),
            V((n_tp,) + w_out.shape, bf16),
            V((8, w_shift.shape[0]), f32),
            V((n_sp, 4, 2 * part), f32),
            V((n_tp, 4, 2 * part), f32),
            V((n_sp, 4, part), f32),
            V((n_tp, 4, part), f32),
            V((8, width), f32),
            V((8, width), f32),
            V((8, width), f32),
            V((samples, 1, tokens), f32),
            V((samples, ctx_rows, LANES), f32),
            V((samples, proj, LANES), f32),
            V((8, 2 * HEAD), f32),
            V((samples, heads, LANES, tokens), bf16),
            V((samples, padded, LANES), bf16),
            V((samples, HEAD + ONES, padded), bf16),
            V((samples, ctx_all, LANES), bf16),
            V((samples, HEAD + ONES, ctx_all), bf16),
            V((2, WINDOW, LANES), f32),
            V((keys, 2 * LANES), f32),
            V((keys, 2 * LANES), f32),
            V((samples, n_tp, block, q_cols), bf16),
            V((n_tp, samples, block, q_cols), bf16),
            dma((8 + samples,)),
            dma((n_sp,)),
            dma((n_sp,)),
            dma((n_tp,)),
            dma((n_tp,)),
            dma((n_sp,)),
            dma((n_sp,)),
            dma((n_tp,)),
            dma((n_tp,)),
            dma((samples, n_sp)),
            dma((samples, n_sp)),
            dma((samples, 2)),
            dma((samples, 2)),
            dma((samples, n_tp)),
            dma((samples, n_tp)),
            dma((n_tp,)),
            dma((n_tp,)),
            dma((n_tp, n_dp)),
            dma((n_tp, n_dp)),
        ],
        compiler_params=pltpu.CompilerParams(
            collective_id=0, has_side_effects=True, vmem_limit_bytes=60 * 1024 * 1024
        ),
    )(
        latent,
        context,
        condition,
        ctx_cond,
        norm_gain.reshape(1, -1),
        w_shift,
        w_scale,
        w_gate,
        w_query,
        w_key.T,
        w_value.T,
        w_out,
        sink_logit,
        ctx_lift,
    )


def solution(mesh):
    return jax.shard_map(
        shards,
        mesh=mesh,
        in_specs=(
            P("dp", "sp", None),
            P("dp", "sp", None),
            P("dp", "sp"),
            P("sp"),
            P(),
            P("sp", "tp"),
            P("sp", "tp"),
            P("sp", "tp"),
            P(None, "tp"),
            P(None, "tp"),
            P(None, "tp"),
            P("tp", None),
            P("tp"),
            P("tp"),
        ),
        out_specs=P("dp", ("sp", "tp"), None),
        check_vma=False,
    )
```

```python
import functools
import math

import jax
import jax.numpy as jnp
from jax import lax
from jax.experimental import pallas as pl
from jax.experimental.pallas import tpu as pltpu
from jax.sharding import PartitionSpec as P

HEAD = 64
WINDOW = 128
GRID_COLS = 64
LANES = 128
ONES = 16
PIECES = 4

epsilon = 1e-06
rope_base = 10000.0
masked_value = -1e30
log2e = 1.4426950408889634
MESH = pl.DeviceIdType.MESH
nt = (((1,), (1,)), ((), ()))
f32 = jnp.float32
bf16 = jnp.bfloat16


def kernel(
    sizes,
    latent,
    context,
    condition,
    ctx_cond,
    norm_gain,
    w_shift,
    w_scale,
    w_gate,
    w_query,
    w_key,
    w_value,
    w_out,
    sink_logit,
    ctx_lift,
    out,
    x_lat,
    x_ctx,
    w_mod,
    w_q,
    w_t,
    w_s,
    w_c,
    cos_row,
    sin_row,
    cos_col,
    sin_col,
    w_o,
    act,
    mod_rx,
    mod_all,
    gate_rx,
    gate_all,
    vec_a,
    vec_b,
    vec_g,
    inv_lat,
    inv_ctx,
    bias_col,
    bias_row,
    q_buf,
    kv_buf,
    vt_buf,
    ckv_buf,
    cvt_buf,
    mask_buf,
    s_a,
    s_b,
    att_buf,
    rows_rx,
    ld_sem,
    ma_send,
    ma_recv,
    mb_send,
    mb_recv,
    ga_send,
    ga_recv,
    gb_send,
    gb_recv,
    cx_send,
    cx_recv,
    ha_send,
    ha_recv,
    at_send,
    at_recv,
    wo_send,
    wo_recv,
    wf_send,
    wf_recv,
):
    n_sp, n_tp, n_dp = sizes
    me_sp, me_tp, me_dp = lax.axis_index("sp"), lax.axis_index("tp"), lax.axis_index("dp")
    samples, tokens, width = latent.shape
    ctx_rows = context.shape[1]
    ctx_all = n_sp * ctx_rows
    part = w_shift.shape[1]
    q_cols = w_query.shape[1]
    heads = q_cols // HEAD
    block = tokens // n_tp
    quarter = HEAD // 4
    q_scale = log2e * HEAD ** (-0.5)

    def other(me, step, count):
        return lax.rem(me + step, count)

    barrier = pltpu.get_barrier_semaphore()
    for axis, me, count in (("sp", me_sp, n_sp), ("tp", me_tp, n_tp), ("dp", me_dp, n_dp)):
        for step in range(1, count):
            pl.semaphore_signal(
                barrier, inc=1, device_id={axis: other(me, step, count)}, device_id_type=MESH
            )

    loads = []
    for source, target in (
        (w_shift, w_mod.at[0]),
        (w_scale, w_mod.at[1]),
        (context, x_ctx),
        (w_key, w_t.at[q_cols : q_cols + HEAD]),
        (w_value, w_t.at[q_cols + HEAD : q_cols + 2 * HEAD]),
        (w_query, w_q),
        (w_gate, w_mod.at[2]),
        *((latent.at[s], x_lat.at[s]) for s in range(samples)),
        (w_out, w_o.at[me_tp]),
    ):
        copy = pltpu.make_async_copy(source, target, ld_sem.at[len(loads)])
        copy.start()
        loads.append(copy)

    def peers(axis, me, count, buffer, send, recv):
        def copy(step, source):
            return pltpu.make_async_remote_copy(
                src_ref=buffer.at[source],
                dst_ref=buffer.at[source],
                send_sem=send.at[step],
                recv_sem=recv.at[step],
                device_id={axis: other(me, step, count)},
                device_id_type=MESH,
            )

        def start():
            for step in range(1, count):
                copy(step, me).start()

        def arrive():
            for step in range(1, count):
                copy(step, other(me, count - step, count)).wait_recv()

        def finish():
            for step in range(1, count):
                copy(step, me).wait_send()

        return start, arrive, finish

    mod_a = peers("sp", me_sp, n_sp, mod_rx, ma_send, ma_recv)
    mod_b = peers("tp", me_tp, n_tp, mod_all, mb_send, mb_recv)
    gate_a = peers("sp", me_sp, n_sp, gate_rx, ga_send, ga_recv)
    gate_b = peers("tp", me_tp, n_tp, gate_all, gb_send, gb_recv)
    keep_rows = mod_rx.shape[1]

    share = w_out.shape[0] // n_dp
    piece = share // PIECES
    across = me_tp + 1 - 2 * lax.rem(me_tp, 2)
    along = lax.rem(me_tp + 2, n_tp)
    diagonal = lax.rem(across + 2, n_tp)

    def piece_copy(kind, i, source, target, local):
        rows = pl.ds(pl.multiple_of(me_dp * share + i * piece, piece), piece)
        return pltpu.make_async_remote_copy(
            src_ref=local.at[rows, :],
            dst_ref=w_o.at[source, rows, :],
            send_sem=wo_send.at[kind, i],
            recv_sem=wo_recv.at[kind, i],
            device_id={"tp": target},
            device_id_type=MESH,
        )

    def own_copy(kind, i):
        return piece_copy(kind, i, me_tp, (across, along)[kind], w_out)

    def relay_copy(i):
        source, target = ((across, along), (along, across))[2 * i // PIECES]
        return piece_copy(2, i, source, target, w_o.at[source])

    def piece_arrive(kind, i):
        source = (across, along, diagonal)[kind]
        target = (across, along, (along, across)[2 * i // PIECES])[kind]
        piece_copy(kind, i, source, target, w_o.at[source]).wait_recv()

    def relay(first, last):
        for i in range(first, last):
            piece_arrive(2 * i // PIECES, i)
            relay_copy(i).start()

    def forward_copy(source, index, hop, part_id):
        rows = pl.ds(pl.multiple_of(part_id * share, share), share)
        return pltpu.make_async_remote_copy(
            src_ref=w_o.at[source, rows, :],
            dst_ref=w_o.at[source, rows, :],
            send_sem=wf_send.at[index, hop],
            recv_sem=wf_recv.at[index, hop],
            device_id={"dp": other(me_dp, hop, n_dp)},
            device_id_type=MESH,
        )

    act[...] = jnp.zeros_like(act)
    cond = condition[...].astype(f32)
    act[0:samples, :] = cond / (1.0 + jnp.exp(-cond))
    cond = ctx_cond[...].astype(f32).reshape(1, -1)
    act[samples : samples + 1, :] = cond / (1.0 + jnp.exp(-cond))
    active = act[...].astype(bf16)
    for i in range(2):
        loads[i].wait()
        mod_rx[me_sp, :, i * part : (i + 1) * part] = jnp.dot(
            active, w_mod[i], preferred_element_type=f32
        )[0:keep_rows]
    pl.semaphore_wait(barrier, n_sp + n_tp + n_dp - 3)
    mod_a[0]()
    own_copy(0, 0).start()
    own_copy(1, 0).start()

    loads[6].wait()
    gate_rx[me_sp] = jnp.dot(active, w_mod[2], preferred_element_type=f32)[0:keep_rows]
    gate_a[0]()

    loads[2].wait()
    for s in range(samples):
        wide = x_ctx[s].astype(f32)
        total = jnp.sum(wide * wide, axis=-1, keepdims=True)
        inv_ctx[s] = jnp.broadcast_to(lax.rsqrt(total / width + epsilon), (ctx_rows, LANES))

    loads[3].wait()
    loads[4].wait()
    loads[5].wait()
    for i in range(0, width, 256):
        w_t[0:q_cols, i : i + 256] = w_q[i : i + 256, :].T

    fill_tables(me_sp * (tokens // GRID_COLS), cos_row, sin_row, cos_col, sin_col)
    key_id = lax.broadcasted_iota(jnp.int32, (WINDOW, LANES), 0)
    query_id = lax.broadcasted_iota(jnp.int32, (WINDOW, LANES), 1)
    mask_buf[0] = jnp.where(key_id >= query_id, 0.0, masked_value)
    mask_buf[1] = jnp.where(key_id <= query_id, 0.0, masked_value)
    q_buf[:, :, HEAD:, :] = jnp.zeros(q_buf.shape[:2] + (LANES - HEAD, tokens), bf16)
    vt_buf[:, HEAD:, :] = jnp.ones((samples, ONES, vt_buf.shape[2]), bf16)
    cvt_buf[:, HEAD:, :] = jnp.ones((samples, ONES, ctx_all), bf16)
    vec_b[...] = jnp.zeros_like(vec_b)

    def stats(s):
        def body(i, carry):
            rows = pl.ds(pl.multiple_of(i * block, block), block)
            wide = x_lat[s, rows, :].astype(f32)
            acc = wide[:, 0:LANES] * wide[:, 0:LANES]
            for k in range(LANES, width, LANES):
                acc = acc + wide[:, k : k + LANES] * wide[:, k : k + LANES]
            total = jnp.sum(acc.T, axis=0, keepdims=True)
            inv_lat[s, :, rows] = lax.rsqrt(total / width + epsilon)
            return carry

        lax.fori_loop(0, n_tp, body, 0)

    loads[7].wait()
    stats(0)

    mod_a[1]()
    total = mod_rx[0]
    for i in range(1, n_sp):
        total = total + mod_rx[i]
    mod_all[me_tp] = total
    mod_b[0]()
    for i in range(1, PIECES):
        own_copy(0, i).start()
        own_copy(1, i).start()

    for s in range(1, samples):
        loads[7 + s].wait()
        stats(s)

    gate_a[1]()
    total = gate_rx[0]
    for i in range(1, n_sp):
        total = total + gate_rx[i]
    gate_all[me_tp] = total
    gate_b[0]()

    mod_b[1]()
    for t in range(n_tp):
        cols = slice(t * part, (t + 1) * part)
        vec_b[0:keep_rows, cols] = mod_all[t, :, 0:part]
        vec_a[0:keep_rows, cols] = (1.0 + mod_all[t, :, part : 2 * part]) * norm_gain[:, cols]

    def fold(target, first, last, base, row):
        gain = vec_a[row : row + 1, :]
        for r in range(first, last, 32):
            target[r - base : r - base + 32, :] = (w_t[r : r + 32, :].astype(f32) * gain).astype(bf16)

    shift = vec_b[...]
    high = shift.astype(bf16).astype(f32)
    shift_pair = jnp.concatenate([high, shift - high], axis=0).astype(bf16)
    bias = lax.dot_general(shift_pair, w_t[q_cols:, :], nt, preferred_element_type=f32)
    bias_row[...] = bias[0:8] + bias[8:16]
    fold(w_c, q_cols, q_cols + 2 * HEAD, q_cols, samples)

    def ctx_copy(s, step, source):
        rows = pl.ds(pl.multiple_of(source * ctx_rows, ctx_rows), ctx_rows)
        return pltpu.make_async_remote_copy(
            src_ref=ckv_buf.at[s, rows, :],
            dst_ref=ckv_buf.at[s, rows, :],
            send_sem=cx_send.at[s, step],
            recv_sem=cx_recv.at[s, step],
            device_id={"sp": other(me_sp, step, n_sp)},
            device_id_type=MESH,
        )

    def context_keys(s):
        rows = pl.ds(pl.multiple_of(me_sp * ctx_rows, ctx_rows), ctx_rows)
        kv = lax.dot_general(x_ctx[s], w_c[...], nt, preferred_element_type=f32)
        ckv_buf[s, rows, :] = (kv * inv_ctx[s] + bias_row[samples : samples + 1, :]).astype(bf16)
        for step in range(1, n_sp):
            ctx_copy(s, step, me_sp).start()

    context_keys(0)

    def fold_sample(s):
        fold(w_s.at[s], 0, q_cols + 2 * HEAD, 0, s)
        bias_col[s, 0:q_cols, :] = jnp.broadcast_to(column[0:q_cols, s : s + 1] * q_scale, (q_cols, LANES))
        bias_col[s, q_cols:, :] = jnp.broadcast_to(column[q_cols:, s : s + 1], (2 * HEAD, LANES))

    bias = lax.dot_general(shift_pair, w_t[0:q_cols, :], nt, preferred_element_type=f32)
    bias = jnp.concatenate([bias[0:8] + bias[8:16], bias_row[...]], axis=1)
    bias = jnp.concatenate([bias, jnp.zeros((LANES - 8, bias.shape[1]), f32)], axis=0)
    column = bias.T

    def halo_copy(s, side):
        source, target = ((tokens, 0), (WINDOW, WINDOW + tokens))[side]
        step = (1, n_sp - 1)[side]
        return pltpu.make_async_remote_copy(
            src_ref=kv_buf.at[s, pl.ds(source, WINDOW), :],
            dst_ref=kv_buf.at[s, pl.ds(target, WINDOW), :],
            send_sem=ha_send.at[s, side],
            recv_sem=ha_recv.at[s, side],
            device_id={"sp": other(me_sp, step, n_sp)},
            device_id_type=MESH,
        )

    def project(s, start):
        cols = slice(start, start + block)
        y = lax.dot_general(w_s[s], x_lat[s, cols, :], nt, preferred_element_type=f32)
        inv = inv_lat[s, :, cols]
        inv_q = inv * q_scale
        cr, sr = cos_row[:, cols], sin_row[:, cols]
        cc, sc = cos_col[...], sin_col[...]

        def wide(first, count):
            return jnp.concatenate([bias_col[s, first : first + count, :]] * (block // LANES), axis=1)

        def rotated(base, scale):
            u = [
                y[base + k * quarter : base + (k + 1) * quarter] * scale
                + wide(base + k * quarter, quarter)
                for k in range(4)
            ]
            return (
                u[0] * cr - u[1] * sr,
                u[0] * sr + u[1] * cr,
                u[2] * cc - u[3] * sc,
                u[2] * sc + u[3] * cc,
            )

        for h in range(heads):
            q_buf[s, h, 0:HEAD, cols] = jnp.concatenate(rotated(h * HEAD, inv_q), axis=0).astype(bf16)
        v = y[q_cols + HEAD :] * inv + wide(q_cols + HEAD, HEAD)
        kv = jnp.concatenate((*rotated(q_cols, inv), v), axis=0)
        vt_buf[s, 0:HEAD, WINDOW + start : WINDOW + start + block] = v.astype(bf16)
        kv_buf[s, WINDOW + start : WINDOW + start + block, :] = kv.T.astype(bf16)

    for s in range(samples):
        if s > 0:
            context_keys(s)
        fold_sample(s)
        for i in range(n_tp):
            project(s, i * block)
        halo_copy(s, 0).start()
        halo_copy(s, 1).start()
        if s < 2:
            relay(s * PIECES // 2, (s + 1) * PIECES // 2)

    def rows_copy(s, step, source):
        target = other(me_tp, step, n_tp)
        return pltpu.make_async_remote_copy(
            src_ref=att_buf.at[s, target],
            dst_ref=rows_rx.at[source, s],
            send_sem=at_send.at[s, step],
            recv_sem=at_recv.at[s, step],
            device_id={"tp": target},
            device_id_type=MESH,
        )

    pairs = heads // 2
    halves = block // LANES
    near_rows = LANES + 2 * WINDOW
    low = lax.broadcasted_iota(jnp.int32, (1, 2 * LANES), 1) < LANES

    def two(ref, pair):
        return jnp.where(low, ref[2 * pair], ref[2 * pair + 1]) * log2e

    def start_of(index):
        step = index // halves + 1
        owner = other(me_tp, step, n_tp)
        return pl.multiple_of(owner * block + (index % halves) * LANES, LANES)

    chunks = [(False, 0, 2 * WINDOW), (False, 2 * WINDOW, LANES)]
    far_chunk = min(256, ctx_all)
    for c in range(0, ctx_all, far_chunk):
        chunks.append((True, c, far_chunk))

    def score_steps(s, index, pair, buf, state):
        start = start_of(index)
        cols = pl.ds(start, LANES)
        q = jnp.concatenate(
            [q_buf[s, 2 * pair, :, cols], q_buf[s, 2 * pair + 1, :, cols]], axis=1
        )
        tops = [None, None]

        def one(chunk):
            far, first, count = chunk
            if far:
                keys = ckv_buf[s, first : first + count, :]
            else:
                keys = kv_buf[s, pl.ds(start + first, count), :]
            scores = jnp.dot(keys, q, preferred_element_type=f32)
            base = near_rows + first if far else first
            if not far:
                mask = mask_buf[0 if first == 0 else 1]
                mask = jnp.concatenate([mask, mask], axis=1)
                edge = scores[0:WINDOW] + mask
                if count > WINDOW:
                    scores = jnp.concatenate([edge, scores[WINDOW:]], axis=0)
                else:
                    scores = edge
            buf[base : base + count, :] = scores
            high = jnp.max(scores.reshape(count // 8, 8, 2 * LANES), axis=0)
            tops[far] = high if tops[far] is None else jnp.maximum(tops[far], high)

        for chunk in chunks:
            yield functools.partial(one, chunk)

        def close():
            near_top = jnp.max(tops[0], axis=0, keepdims=True)
            far_top = jnp.max(tops[1], axis=0, keepdims=True)
            lift = two(ctx_lift, pair)
            state.append(
                jnp.maximum(jnp.maximum(near_top, far_top + lift), two(sink_logit, pair))
            )

        yield close

    def value_steps(s, index, pair, buf, top):
        start = start_of(index)
        far_top = top - two(ctx_lift, pair)
        acc = [None]

        def one(chunk):
            far, first, count = chunk
            base = near_rows + first if far else first
            p = jnp.exp2(buf[base : base + count, :] - (far_top if far else top)).astype(bf16)
            if far:
                values = cvt_buf[s, :, first : first + count]
            else:
                values = vt_buf[s, :, pl.ds(start + first, count)]
            term = jnp.dot(values, p, preferred_element_type=f32)
            acc[0] = term if acc[0] is None else acc[0] + term

        for chunk in chunks:
            yield functools.partial(one, chunk)

        def close():
            weight = acc[0][HEAD : HEAD + 1] + jnp.exp2(two(sink_logit, pair) - top)
            rows = acc[0][0:HEAD] * (1.0 / weight)
            stacked = jnp.concatenate([rows[:, 0:LANES], rows[:, LANES:]], axis=0)
            owner = other(me_tp, index // halves + 1, n_tp)
            half = pl.multiple_of((index % halves) * LANES, LANES)
            att_buf[s, owner, pl.ds(half, LANES), pair * LANES : (pair + 1) * LANES] = (
                stacked.T.astype(bf16)
            )

        yield close

    def run(*streams):
        for steps in zip(*streams):
            for step in steps:
                step()

    bufs = (s_a, s_b)

    def attention(s):
        count = n_tp * halves
        top0 = []
        run(score_steps(s, 0, 0, s_a, top0))

        def body(index, top, last):
            for pair in range(pairs):
                mine_buf, next_buf = bufs[pair % 2], bufs[(pair + 1) % 2]
                fresh = []
                streams = [value_steps(s, index, pair, mine_buf, top)]
                if pair + 1 < pairs:
                    streams.insert(0, score_steps(s, index, pair + 1, next_buf, fresh))
                elif not last:
                    streams.insert(0, score_steps(s, index + 1, 0, next_buf, fresh))
                run(*streams)
                top = fresh[0] if fresh else top

            step = index // halves + 1

            @pl.when((index % halves == halves - 1) & (step < n_tp))
            def _():
                rows_copy(s, step, me_tp).start()

            return top

        top = lax.fori_loop(0, count - 1, lambda i, top: body(i, top, False), top0[0])
        body(count - 1, top, True)
        rows_rx[me_tp, s] = att_buf[s, me_tp]

    def context_ready(s):
        for step in range(1, n_sp):
            ctx_copy(s, step, other(me_sp, n_sp - step, n_sp)).wait_recv()
        for c in range(0, ctx_all, 256):
            cvt_buf[s, 0:HEAD, c : c + 256] = ckv_buf[s, c : c + 256, :].T[HEAD:]

    def halo_ready(s):
        for side in range(2):
            halo_copy(s, side).wait_recv()
            first = (0, WINDOW + tokens)[side]
            valid = (me_sp > 0, me_sp < n_sp - 1)[side]
            rows = jnp.where(valid, kv_buf[s, first : first + WINDOW, :].astype(f32), 0.0)
            kv_buf[s, first : first + WINDOW, :] = rows.astype(bf16)
            vt_buf[s, 0:HEAD, first : first + WINDOW] = rows.T[HEAD:].astype(bf16)
            vt_buf[s, HEAD:, first : first + WINDOW] = jnp.where(
                valid, jnp.ones((ONES, WINDOW), f32), 0.0
            ).astype(bf16)

    for s in range(samples):
        halo_ready(s)
        context_ready(s)
        attention(s)
        if s == 0:
            for index, source in enumerate((across, along, diagonal)):
                for i in range(PIECES):
                    if index == 2 or 2 * i // PIECES != index:
                        piece_arrive(index, i)
                for hop in range(1, n_dp):
                    forward_copy(source, index, hop, me_dp).start()

    gate_b[1]()
    for t in range(n_tp):
        vec_g[0:keep_rows, t * part : (t + 1) * part] = gate_all[t]

    loads[-1].wait()
    for index, source in enumerate((across, along, diagonal)):
        for hop in range(1, n_dp):
            forward_copy(source, index, hop, other(me_dp, n_dp - hop, n_dp)).wait_recv()
    chunk = 512
    for s in range(samples):
        for step in range(1, n_tp):
            rows_copy(s, step, other(me_tp, n_tp - step, n_tp)).wait_recv()

        def finish(i, carry):
            cols = pl.ds(pl.multiple_of(i * chunk, chunk), chunk)
            acc = jnp.dot(rows_rx[0, s], w_o[0, :, cols], preferred_element_type=f32)
            for t in range(1, n_tp):
                acc += jnp.dot(rows_rx[t, s], w_o[t, :, cols], preferred_element_type=f32)
            out[s, :, cols] = (acc * vec_g[s : s + 1, cols]).astype(bf16)
            return carry

        lax.fori_loop(0, width // chunk, finish, 0)

    for _, _, finish_send in (mod_a, mod_b, gate_a, gate_b):
        finish_send()
    for s in range(samples):
        for step in range(1, n_sp):
            ctx_copy(s, step, me_sp).wait_send()
        halo_copy(s, 0).wait_send()
        halo_copy(s, 1).wait_send()
    for i in range(PIECES):
        own_copy(0, i).wait_send()
        own_copy(1, i).wait_send()
        relay_copy(i).wait_send()
    for index, source in enumerate((across, along, diagonal)):
        for hop in range(1, n_dp):
            forward_copy(source, index, hop, me_dp).wait_send()
    for step in range(1, n_tp):
        for s in range(samples):
            rows_copy(s, step, me_tp).wait_send()


def fill_tables(first_row, cos_row, sin_row, cos_col, sin_col):
    tokens = cos_row.shape[1]
    quarter = HEAD // 4

    def pair(ticks, shape):
        power = lax.broadcasted_iota(jnp.int32, shape, 0).astype(f32)
        angles = ticks.astype(f32) * jnp.exp(power * (-math.log(rope_base) / quarter))
        return jnp.cos(angles), jnp.sin(angles)

    shape = cos_col.shape
    token = lax.broadcasted_iota(jnp.int32, shape, 1)
    cos_col[...], sin_col[...] = pair(token % GRID_COLS, shape)
    lines = tokens // GRID_COLS
    shape = (quarter, LANES)
    for first in range(0, lines, LANES):
        line = lax.broadcasted_iota(jnp.int32, shape, 1) + first + first_row
        cos_all, sin_all = pair(line, shape)
        half = lax.broadcasted_iota(jnp.int32, shape, 1) < GRID_COLS
        for r in range(0, min(LANES, lines - first), 2):
            cols = slice((first + r) * GRID_COLS, (first + r + 2) * GRID_COLS)
            for source, target in ((cos_all, cos_row), (sin_all, sin_row)):
                target[:, cols] = jnp.where(half, source[:, r : r + 1], source[:, r + 1 : r + 2])


def shards(
    latent,
    context,
    condition,
    ctx_cond,
    norm_gain,
    w_shift,
    w_scale,
    w_gate,
    w_query,
    w_key,
    w_value,
    w_out,
    sink_logit,
    ctx_lift,
):
    samples, tokens, width = latent.shape
    ctx_rows = context.shape[1]
    n_sp, n_tp, n_dp = lax.axis_size("sp"), lax.axis_size("tp"), lax.axis_size("dp")
    q_cols = w_query.shape[1]
    heads = q_cols // HEAD
    assert w_key.shape[1] == HEAD and tokens % GRID_COLS == 0 and samples < 4 and heads % 4 == 0 and n_tp == 4 and samples == 2
    part = w_shift.shape[1]
    block = tokens // n_tp
    ctx_all = n_sp * ctx_rows
    vmem = pl.BlockSpec(memory_space=pltpu.VMEM)
    smem = pl.BlockSpec(memory_space=pltpu.SMEM)
    anywhere = pl.BlockSpec(memory_space=pl.ANY)
    dma = pltpu.SemaphoreType.DMA
    padded = tokens + 2 * WINDOW
    proj = q_cols + 2 * HEAD
    keys = LANES + 2 * WINDOW + ctx_all
    V = pltpu.VMEM
    return pl.pallas_call(
        functools.partial(kernel, (n_sp, n_tp, n_dp)),
        out_shape=V((samples, block, width), bf16),
        in_specs=[anywhere] * 2 + [vmem] * 3 + [anywhere] * 7 + [smem] * 2,
        out_specs=vmem,
        scratch_shapes=[
            V(latent.shape, bf16),
            V(context.shape, bf16),
            V((3,) + w_shift.shape, bf16),
            V(w_query.shape, bf16),
            V((proj, width), bf16),
            V((samples, proj, width), bf16),
            V((2 * HEAD, width), bf16),
            V((HEAD // 4, tokens), f32),
            V((HEAD // 4, tokens), f32),
            V((HEAD // 4, block), f32),
            V((HEAD // 4, block), f32),
            V((n_tp,) + w_out.shape, bf16),
            V((8, w_shift.shape[0]), f32),
            V((n_sp, 4, 2 * part), f32),
            V((n_tp, 4, 2 * part), f32),
            V((n_sp, 4, part), f32),
            V((n_tp, 4, part), f32),
            V((8, width), f32),
            V((8, width), f32),
            V((8, width), f32),
            V((samples, 1, tokens), f32),
            V((samples, ctx_rows, LANES), f32),
            V((samples, proj, LANES), f32),
            V((8, 2 * HEAD), f32),
            V((samples, heads, LANES, tokens), bf16),
            V((samples, padded, LANES), bf16),
            V((samples, HEAD + ONES, padded), bf16),
            V((samples, ctx_all, LANES), bf16),
            V((samples, HEAD + ONES, ctx_all), bf16),
            V((2, WINDOW, LANES), f32),
            V((keys, 2 * LANES), f32),
            V((keys, 2 * LANES), f32),
            V((samples, n_tp, block, q_cols), bf16),
            V((n_tp, samples, block, q_cols), bf16),
            dma((8 + samples,)),
            dma((n_sp,)),
            dma((n_sp,)),
            dma((n_tp,)),
            dma((n_tp,)),
            dma((n_sp,)),
            dma((n_sp,)),
            dma((n_tp,)),
            dma((n_tp,)),
            dma((samples, n_sp)),
            dma((samples, n_sp)),
            dma((samples, 2)),
            dma((samples, 2)),
            dma((samples, n_tp)),
            dma((samples, n_tp)),
            dma((3, PIECES)),
            dma((3, PIECES)),
            dma((3, n_dp)),
            dma((3, n_dp)),
        ],
        compiler_params=pltpu.CompilerParams(
            collective_id=0, has_side_effects=True, vmem_limit_bytes=56 * 1024 * 1024
        ),
    )(
        latent,
        context,
        condition,
        ctx_cond,
        norm_gain.reshape(1, -1),
        w_shift,
        w_scale,
        w_gate,
        w_query,
        w_key.T,
        w_value.T,
        w_out,
        sink_logit,
        ctx_lift,
    )


def solution(mesh):
    return jax.shard_map(
        shards,
        mesh=mesh,
        in_specs=(
            P("dp", "sp", None),
            P("dp", "sp", None),
            P("dp", "sp"),
            P("sp"),
            P(),
            P("sp", "tp"),
            P("sp", "tp"),
            P("sp", "tp"),
            P(None, "tp"),
            P(None, "tp"),
            P(None, "tp"),
            P("tp", None),
            P("tp"),
            P("tp"),
        ),
        out_specs=P("dp", ("sp", "tp"), None),
        check_vma=False,
    )
```

```python
import functools
import math

import jax
import jax.numpy as jnp
from jax import lax
from jax.experimental import pallas as pl
from jax.experimental.pallas import tpu as pltpu
from jax.sharding import PartitionSpec as P

HEAD = 64
WINDOW = 128
GRID_COLS = 64
LANES = 128
ONES = 16
PIECES = 4
AHEAD = 2

epsilon = 1e-06
rope_base = 10000.0
masked_value = -1e30
log2e = 1.4426950408889634
MESH = pl.DeviceIdType.MESH
nt = (((1,), (1,)), ((), ()))
f32 = jnp.float32
bf16 = jnp.bfloat16


def kernel(
    sizes,
    latent,
    context,
    condition_in,
    ctx_cond_in,
    norm_gain_in,
    w_shift,
    w_scale,
    w_gate,
    w_query,
    w_key,
    w_value,
    w_out,
    sink_logit_in,
    ctx_lift_in,
    out,
    condition,
    ctx_cond,
    norm_gain,
    sink_logit,
    ctx_lift,
    x_lat,
    x_ctx,
    w_mod,
    w_q,
    w_t,
    w_s,
    w_c,
    cos_row,
    sin_row,
    cos_col,
    sin_col,
    w_o,
    act,
    mod_rx,
    mod_all,
    gate_rx,
    gate_all,
    vec_a,
    vec_b,
    vec_g,
    inv_lat,
    inv_ctx,
    bias_col,
    bias_row,
    q_buf,
    kv_buf,
    vt_buf,
    ckv_buf,
    cvt_buf,
    mask_buf,
    s_a,
    s_b,
    s_c,
    s_d,
    att_buf,
    rows_rx,
    mix_buf,
    ld_sem,
    ma_send,
    ma_recv,
    mb_send,
    mb_recv,
    ga_send,
    ga_recv,
    gb_send,
    gb_recv,
    cx_send,
    cx_recv,
    ha_send,
    ha_recv,
    at_send,
    at_recv,
    wo_send,
    wo_recv,
    wf_send,
    wf_recv,
):
    n_sp, n_tp, n_dp = sizes
    me_sp, me_tp, me_dp = lax.axis_index("sp"), lax.axis_index("tp"), lax.axis_index("dp")
    samples, tokens, width = latent.shape
    ctx_rows = context.shape[1]
    ctx_all = n_sp * ctx_rows
    part = w_shift.shape[1]
    q_cols = w_query.shape[1]
    heads = q_cols // HEAD
    block = tokens // n_tp
    quarter = HEAD // 4
    q_scale = log2e * HEAD ** (-0.5)

    def other(me, step, count):
        return lax.rem(me + step, count)

    barrier = pltpu.get_barrier_semaphore()
    for axis, me, count in (("sp", me_sp, n_sp), ("tp", me_tp, n_tp), ("dp", me_dp, n_dp)):
        for step in range(1, count):
            pl.semaphore_signal(
                barrier, inc=1, device_id={axis: other(me, step, count)}, device_id_type=MESH
            )

    loads = []
    for source, target in (
        (condition_in, condition),
        (ctx_cond_in, ctx_cond),
        (w_shift, w_mod.at[0]),
        (w_scale, w_mod.at[1]),
        (context, x_ctx),
        (w_key, w_t.at[q_cols : q_cols + HEAD]),
        (w_value, w_t.at[q_cols + HEAD : q_cols + 2 * HEAD]),
        (w_query, w_q),
        (w_gate, w_mod.at[2]),
        *((latent.at[s], x_lat.at[s]) for s in range(samples)),
        (norm_gain_in, norm_gain),
        (sink_logit_in, sink_logit),
        (ctx_lift_in, ctx_lift),
        (w_out, w_o.at[me_tp]),
    ):
        copy = pltpu.make_async_copy(source, target, ld_sem.at[len(loads)])
        copy.start()
        loads.append(copy)

    def peers(axis, me, count, buffer, send, recv):
        def copy(step, source):
            return pltpu.make_async_remote_copy(
                src_ref=buffer.at[source],
                dst_ref=buffer.at[source],
                send_sem=send.at[step],
                recv_sem=recv.at[step],
                device_id={axis: other(me, step, count)},
                device_id_type=MESH,
            )

        def start():
            for step in range(1, count):
                copy(step, me).start()

        def arrive():
            for step in range(1, count):
                copy(step, other(me, count - step, count)).wait_recv()

        def finish():
            for step in range(1, count):
                copy(step, me).wait_send()

        return start, arrive, finish

    mod_a = peers("sp", me_sp, n_sp, mod_rx, ma_send, ma_recv)
    mod_b = peers("tp", me_tp, n_tp, mod_all, mb_send, mb_recv)
    gate_a = peers("sp", me_sp, n_sp, gate_rx, ga_send, ga_recv)
    gate_b = peers("tp", me_tp, n_tp, gate_all, gb_send, gb_recv)
    keep_rows = mod_rx.shape[1]

    share = w_out.shape[0] // n_dp
    piece = share // PIECES
    across = me_tp + 1 - 2 * lax.rem(me_tp, 2)
    along = lax.rem(me_tp + 2, n_tp)
    diagonal = lax.rem(across + 2, n_tp)

    def piece_copy(kind, i, source, target, local):
        rows = pl.ds(pl.multiple_of(me_dp * share + i * piece, piece), piece)
        return pltpu.make_async_remote_copy(
            src_ref=local.at[rows, :],
            dst_ref=w_o.at[source, rows, :],
            send_sem=wo_send.at[kind, i],
            recv_sem=wo_recv.at[kind, i],
            device_id={"tp": target},
            device_id_type=MESH,
        )

    def own_copy(kind, i):
        return piece_copy(kind, i, me_tp, (across, along)[kind], w_out)

    def relay_copy(i):
        source, target = ((across, along), (along, across))[2 * i // PIECES]
        return piece_copy(2, i, source, target, w_o.at[source])

    def piece_arrive(kind, i):
        source = (across, along, diagonal)[kind]
        target = (across, along, (along, across)[2 * i // PIECES])[kind]
        piece_copy(kind, i, source, target, w_o.at[source]).wait_recv()

    def relay(first, last):
        for i in range(first, last):
            piece_arrive(2 * i // PIECES, i)
            relay_copy(i).start()

    def forward_copy(source, index, hop, part_id):
        rows = pl.ds(pl.multiple_of(part_id * share, share), share)
        return pltpu.make_async_remote_copy(
            src_ref=w_o.at[source, rows, :],
            dst_ref=w_o.at[source, rows, :],
            send_sem=wf_send.at[index, hop],
            recv_sem=wf_recv.at[index, hop],
            device_id={"dp": other(me_dp, hop, n_dp)},
            device_id_type=MESH,
        )

    act[...] = jnp.zeros_like(act)
    loads[0].wait()
    loads[1].wait()
    cond = condition[...].astype(f32)
    act[0:samples, :] = cond / (1.0 + jnp.exp(-cond))
    cond = ctx_cond[...].astype(f32).reshape(1, -1)
    act[samples : samples + 1, :] = cond / (1.0 + jnp.exp(-cond))
    active = act[...].astype(bf16)
    for i in range(2):
        loads[2 + i].wait()
        mod_rx[me_sp, :, i * part : (i + 1) * part] = jnp.dot(
            active, w_mod[i], preferred_element_type=f32
        )[0:keep_rows]
    pl.semaphore_wait(barrier, n_sp + n_tp + n_dp - 3)
    mod_a[0]()
    own_copy(0, 0).start()
    own_copy(1, 0).start()

    loads[8].wait()
    gate_rx[me_sp] = jnp.dot(active, w_mod[2], preferred_element_type=f32)[0:keep_rows]
    gate_a[0]()

    loads[4].wait()
    for s in range(samples):
        wide = x_ctx[s].astype(f32)
        total = jnp.sum(wide * wide, axis=-1, keepdims=True)
        inv_ctx[s] = jnp.broadcast_to(lax.rsqrt(total / width + epsilon), (ctx_rows, LANES))

    loads[5].wait()
    loads[6].wait()
    loads[7].wait()
    for i in range(0, width, 256):
        w_t[0:q_cols, i : i + 256] = w_q[i : i + 256, :].T

    fill_tables(me_sp * (tokens // GRID_COLS), cos_row, sin_row, cos_col, sin_col)
    key_id = lax.broadcasted_iota(jnp.int32, (WINDOW, LANES), 0)
    query_id = lax.broadcasted_iota(jnp.int32, (WINDOW, LANES), 1)
    mask_buf[0] = jnp.where(key_id >= query_id, 0.0, masked_value)
    mask_buf[1] = jnp.where(key_id <= query_id, 0.0, masked_value)
    q_buf[:, :, HEAD:, :] = jnp.zeros(q_buf.shape[:2] + (LANES - HEAD, tokens), bf16)
    vt_buf[:, HEAD:, :] = jnp.ones((samples, ONES, vt_buf.shape[2]), bf16)
    cvt_buf[:, HEAD:, :] = jnp.ones((samples, ONES, ctx_all), bf16)
    vec_b[...] = jnp.zeros_like(vec_b)

    def stats(s):
        def body(i, carry):
            rows = pl.ds(pl.multiple_of(i * block, block), block)
            wide = x_lat[s, rows, :].astype(f32)
            acc = wide[:, 0:LANES] * wide[:, 0:LANES]
            for k in range(LANES, width, LANES):
                acc = acc + wide[:, k : k + LANES] * wide[:, k : k + LANES]
            total = jnp.sum(acc.T, axis=0, keepdims=True)
            inv_lat[s, :, rows] = lax.rsqrt(total / width + epsilon)
            return carry

        lax.fori_loop(0, n_tp, body, 0)

    loads[9].wait()
    stats(0)

    mod_a[1]()
    total = mod_rx[0]
    for i in range(1, n_sp):
        total = total + mod_rx[i]
    mod_all[me_tp] = total
    mod_b[0]()
    for i in range(1, PIECES):
        own_copy(0, i).start()
        own_copy(1, i).start()

    for s in range(1, samples):
        loads[9 + s].wait()
        stats(s)

    gate_a[1]()
    total = gate_rx[0]
    for i in range(1, n_sp):
        total = total + gate_rx[i]
    gate_all[me_tp] = total
    gate_b[0]()

    for i in range(2, 5):
        loads[-i].wait()

    mod_b[1]()
    for t in range(n_tp):
        cols = slice(t * part, (t + 1) * part)
        vec_b[0:keep_rows, cols] = mod_all[t, :, 0:part]
        vec_a[0:keep_rows, cols] = (1.0 + mod_all[t, :, part : 2 * part]) * norm_gain[:, cols]

    def fold(target, first, last, base, row):
        gain = vec_a[row : row + 1, :]
        for r in range(first, last, 32):
            target[r - base : r - base + 32, :] = (w_t[r : r + 32, :].astype(f32) * gain).astype(bf16)

    shift = vec_b[...]
    high = shift.astype(bf16).astype(f32)
    shift_pair = jnp.concatenate([high, shift - high], axis=0).astype(bf16)
    bias = lax.dot_general(shift_pair, w_t[q_cols:, :], nt, preferred_element_type=f32)
    bias_row[...] = bias[0:8] + bias[8:16]
    fold(w_c, q_cols, q_cols + 2 * HEAD, q_cols, samples)

    def ctx_copy(s, step, source):
        rows = pl.ds(pl.multiple_of(source * ctx_rows, ctx_rows), ctx_rows)
        return pltpu.make_async_remote_copy(
            src_ref=ckv_buf.at[s, rows, :],
            dst_ref=ckv_buf.at[s, rows, :],
            send_sem=cx_send.at[s, step],
            recv_sem=cx_recv.at[s, step],
            device_id={"sp": other(me_sp, step, n_sp)},
            device_id_type=MESH,
        )

    def context_keys(s):
        rows = pl.ds(pl.multiple_of(me_sp * ctx_rows, ctx_rows), ctx_rows)
        kv = lax.dot_general(x_ctx[s], w_c[...], nt, preferred_element_type=f32)
        ckv_buf[s, rows, :] = (kv * inv_ctx[s] + bias_row[samples : samples + 1, :]).astype(bf16)
        for step in range(1, n_sp):
            ctx_copy(s, step, me_sp).start()

    context_keys(0)

    def fold_sample(s):
        fold(w_s.at[s], 0, q_cols + 2 * HEAD, 0, s)
        bias_col[s, 0:q_cols, :] = jnp.broadcast_to(column[0:q_cols, s : s + 1] * q_scale, (q_cols, LANES))
        bias_col[s, q_cols:, :] = jnp.broadcast_to(column[q_cols:, s : s + 1], (2 * HEAD, LANES))

    bias = lax.dot_general(shift_pair, w_t[0:q_cols, :], nt, preferred_element_type=f32)
    bias = jnp.concatenate([bias[0:8] + bias[8:16], bias_row[...]], axis=1)
    bias = jnp.concatenate([bias, jnp.zeros((LANES - 8, bias.shape[1]), f32)], axis=0)
    column = bias.T

    def halo_copy(s, side):
        source, target = ((tokens, 0), (WINDOW, WINDOW + tokens))[side]
        step = (1, n_sp - 1)[side]
        return pltpu.make_async_remote_copy(
            src_ref=kv_buf.at[s, pl.ds(source, WINDOW), :],
            dst_ref=kv_buf.at[s, pl.ds(target, WINDOW), :],
            send_sem=ha_send.at[s, side],
            recv_sem=ha_recv.at[s, side],
            device_id={"sp": other(me_sp, step, n_sp)},
            device_id_type=MESH,
        )

    def project(s, start):
        cols = slice(start, start + block)
        y = lax.dot_general(w_s[s], x_lat[s, cols, :], nt, preferred_element_type=f32)
        inv = inv_lat[s, :, cols]
        inv_q = inv * q_scale
        cr, sr = cos_row[:, cols], sin_row[:, cols]
        cc, sc = cos_col[...], sin_col[...]

        def wide(first, count):
            return jnp.concatenate([bias_col[s, first : first + count, :]] * (block // LANES), axis=1)

        def rotated(base, scale):
            u = [
                y[base + k * quarter : base + (k + 1) * quarter] * scale
                + wide(base + k * quarter, quarter)
                for k in range(4)
            ]
            return (
                u[0] * cr - u[1] * sr,
                u[0] * sr + u[1] * cr,
                u[2] * cc - u[3] * sc,
                u[2] * sc + u[3] * cc,
            )

        for h in range(heads):
            q_buf[s, h, 0:HEAD, cols] = jnp.concatenate(rotated(h * HEAD, inv_q), axis=0).astype(bf16)
        v = y[q_cols + HEAD :] * inv + wide(q_cols + HEAD, HEAD)
        kv = jnp.concatenate((*rotated(q_cols, inv), v), axis=0)
        vt_buf[s, 0:HEAD, WINDOW + start : WINDOW + start + block] = v.astype(bf16)
        kv_buf[s, WINDOW + start : WINDOW + start + block, :] = kv.T.astype(bf16)

    for s in range(samples):
        if s > 0:
            context_keys(s)
        fold_sample(s)
        for i in range(n_tp):
            project(s, i * block)
        halo_copy(s, 0).start()
        halo_copy(s, 1).start()
        if s < 2:
            relay(s * PIECES // 2, (s + 1) * PIECES // 2)

    halves = block // LANES

    def rows_copy(s, step, source):
        target = other(me_tp, step, n_tp)
        return pltpu.make_async_remote_copy(
            src_ref=att_buf.at[s, target],
            dst_ref=rows_rx.at[source, s],
            send_sem=at_send.at[s, step],
            recv_sem=at_recv.at[s, step],
            device_id={"tp": target},
            device_id_type=MESH,
        )

    pairs = heads // 2
    near_rows = LANES + 2 * WINDOW
    low = lax.broadcasted_iota(jnp.int32, (1, 2 * LANES), 1) < LANES

    def two(ref, pair):
        return jnp.where(low, ref[2 * pair], ref[2 * pair + 1]) * log2e

    def start_of(index):
        step = index // halves + 1
        owner = other(me_tp, step, n_tp)
        return pl.multiple_of(owner * block + (index % halves) * LANES, LANES)

    def chunks_of(near, far):
        return [(False, c, min(near, near_rows - c)) for c in range(0, near_rows, near)] + [
            (True, c, min(far, ctx_all)) for c in range(0, ctx_all, min(far, ctx_all))
        ]

    score_chunks = chunks_of(384, 256)
    value_chunks = chunks_of(256, 256)

    def score_steps(s, index, pair, buf, state):
        start = start_of(index)
        cols = pl.ds(start, LANES)
        q = jnp.concatenate(
            [q_buf[s, 2 * pair, :, cols], q_buf[s, 2 * pair + 1, :, cols]], axis=1
        )
        tops = [None, None]

        def one(chunk):
            far, first, count = chunk
            if far:
                keys = ckv_buf[s, first : first + count, :]
            else:
                keys = kv_buf[s, pl.ds(start + first, count), :]
            scores = jnp.dot(keys, q, preferred_element_type=f32)
            base = near_rows + first if far else first
            if not far:
                parts = [scores[r : r + WINDOW] for r in range(0, count, WINDOW)]
                for edge, place in ((0, 0), (1, near_rows - WINDOW)):
                    if first <= place < first + count:
                        mask = jnp.concatenate([mask_buf[edge], mask_buf[edge]], axis=1)
                        parts[(place - first) // WINDOW] += mask
                scores = jnp.concatenate(parts, axis=0)
            buf[base : base + count, :] = scores
            high = jnp.max(scores.reshape(count // 8, 8, 2 * LANES), axis=0)
            tops[far] = high if tops[far] is None else jnp.maximum(tops[far], high)

        for chunk in score_chunks:
            yield functools.partial(one, chunk)

        def close():
            near_top = jnp.max(tops[0], axis=0, keepdims=True)
            far_top = jnp.max(tops[1], axis=0, keepdims=True)
            lift = two(ctx_lift, pair)
            state.append(
                jnp.maximum(jnp.maximum(near_top, far_top + lift), two(sink_logit, pair))
            )

        yield close

    def value_steps(s, index, pair, buf, top):
        start = start_of(index)
        far_top = top - two(ctx_lift, pair)
        acc = [None]

        def one(chunk):
            far, first, count = chunk
            base = near_rows + first if far else first
            p = jnp.exp2(buf[base : base + count, :] - (far_top if far else top)).astype(bf16)
            if far:
                values = cvt_buf[s, :, first : first + count]
            else:
                values = vt_buf[s, :, pl.ds(start + first, count)]
            term = jnp.dot(values, p, preferred_element_type=f32)
            acc[0] = term if acc[0] is None else acc[0] + term

        for chunk in value_chunks:
            yield functools.partial(one, chunk)

        def close():
            weight = acc[0][HEAD : HEAD + 1] + jnp.exp2(two(sink_logit, pair) - top)
            rows = acc[0][0:HEAD] * (1.0 / weight)
            stacked = jnp.concatenate([rows[:, 0:LANES], rows[:, LANES:]], axis=0)
            owner = other(me_tp, index // halves + 1, n_tp)
            half = pl.multiple_of((index % halves) * LANES, LANES)
            att_buf[s, owner, pl.ds(half, LANES), pair * LANES : (pair + 1) * LANES] = (
                stacked.T.astype(bf16)
            )

        yield close

    def run(*streams):
        streams = [list(steps) for steps in streams]
        order = sorted(
            ((i + 1) / len(steps), k, i) for k, steps in enumerate(streams) for i in range(len(steps))
        )
        for _, k, i in order:
            streams[k][i]()

    bufs = (s_a, s_b, s_c, s_d)
    per_step = halves * pairs

    def attention(s):
        def scores_of(unit, base, target):
            return score_steps(s, base + unit // pairs, unit % pairs, bufs[unit % len(bufs)], target)

        tops = [[] for _ in range(AHEAD)]
        run(*(scores_of(unit, 0, tops[unit]) for unit in range(AHEAD)))

        def body(step, tops, last):
            base = step * halves
            known = [[top] for top in tops]
            for unit in range(per_step):
                streams = []
                if not last or unit + AHEAD < per_step:
                    known.append([])
                    streams.append(scores_of(unit + AHEAD, base, known[-1]))
                streams.append(
                    value_steps(
                        s, base + unit // pairs, unit % pairs, bufs[unit % len(bufs)], known[unit][0]
                    )
                )
                run(*streams)
            if not last:
                rows_copy(s, step + 1, me_tp).start()
            return tuple(top[0] for top in known[per_step:])

        tops = tuple(top[0] for top in tops)
        tops = lax.fori_loop(0, n_tp - 1, lambda step, tops: body(step, tops, False), tops)
        body(n_tp - 1, tops, True)
        rows_rx[me_tp, s] = att_buf[s, me_tp]

    def context_ready(s):
        for step in range(1, n_sp):
            ctx_copy(s, step, other(me_sp, n_sp - step, n_sp)).wait_recv()
        for c in range(0, ctx_all, 256):
            cvt_buf[s, 0:HEAD, c : c + 256] = ckv_buf[s, c : c + 256, :].T[HEAD:]

    def halo_ready(s):
        for side in range(2):
            halo_copy(s, side).wait_recv()
            first = (0, WINDOW + tokens)[side]
            valid = (me_sp > 0, me_sp < n_sp - 1)[side]
            rows = jnp.where(valid, kv_buf[s, first : first + WINDOW, :].astype(f32), 0.0)
            kv_buf[s, first : first + WINDOW, :] = rows.astype(bf16)
            vt_buf[s, 0:HEAD, first : first + WINDOW] = rows.T[HEAD:].astype(bf16)
            vt_buf[s, HEAD:, first : first + WINDOW] = jnp.where(
                valid, jnp.ones((ONES, WINDOW), f32), 0.0
            ).astype(bf16)

    for s in range(samples):
        halo_ready(s)
        context_ready(s)
        attention(s)
        if s == 0:
            for index, source in enumerate((across, along, diagonal)):
                for i in range(PIECES):
                    if index == 2 or 2 * i // PIECES != index:
                        piece_arrive(index, i)
                for hop in range(1, n_dp):
                    forward_copy(source, index, hop, me_dp).start()

    gate_b[1]()
    for t in range(n_tp):
        vec_g[0:keep_rows, t * part : (t + 1) * part] = gate_all[t]

    loads[-1].wait()
    for index, source in enumerate((across, along, diagonal)):
        for hop in range(1, n_dp):
            forward_copy(source, index, hop, other(me_dp, n_dp - hop, n_dp)).wait_recv()
    chunk = 512

    def rows_arrive(s, step):
        rows_copy(s, step, other(me_tp, n_tp - step, n_tp)).wait_recv()

    def mix(s, steps, c):
        acc = None
        for step in steps:
            t = other(me_tp, n_tp - step, n_tp)
            term = jnp.dot(rows_rx[t, s], w_o[t, :, c : c + chunk], preferred_element_type=f32)
            acc = term if acc is None else acc + term
        return acc

    for s in range(samples):
        final = s == samples - 1
        for step in range(1, n_tp - 1 if final else n_tp):
            rows_arrive(s, step)
        for c in range(0, width, chunk):
            cols = slice(c, c + chunk)
            if final:
                mix_buf[:, cols] = mix(s, range(n_tp - 1), c)
            else:
                out[s, :, cols] = (mix(s, range(n_tp), c) * vec_g[s : s + 1, cols]).astype(bf16)
    rows_arrive(samples - 1, n_tp - 1)
    for c in range(0, width, chunk):
        cols = slice(c, c + chunk)
        acc = mix_buf[:, cols] + mix(samples - 1, (n_tp - 1,), c)
        out[samples - 1, :, cols] = (acc * vec_g[samples - 1 : samples, cols]).astype(bf16)

    for _, _, finish_send in (mod_a, mod_b, gate_a, gate_b):
        finish_send()
    for s in range(samples):
        for step in range(1, n_sp):
            ctx_copy(s, step, me_sp).wait_send()
        halo_copy(s, 0).wait_send()
        halo_copy(s, 1).wait_send()
    for i in range(PIECES):
        own_copy(0, i).wait_send()
        own_copy(1, i).wait_send()
        relay_copy(i).wait_send()
    for index, source in enumerate((across, along, diagonal)):
        for hop in range(1, n_dp):
            forward_copy(source, index, hop, me_dp).wait_send()
    for step in range(1, n_tp):
        for s in range(samples):
            rows_copy(s, step, me_tp).wait_send()


def fill_tables(first_row, cos_row, sin_row, cos_col, sin_col):
    tokens = cos_row.shape[1]
    quarter = HEAD // 4

    def pair(ticks, shape):
        power = lax.broadcasted_iota(jnp.int32, shape, 0).astype(f32)
        angles = ticks.astype(f32) * jnp.exp(power * (-math.log(rope_base) / quarter))
        return jnp.cos(angles), jnp.sin(angles)

    shape = cos_col.shape
    token = lax.broadcasted_iota(jnp.int32, shape, 1)
    cos_col[...], sin_col[...] = pair(token % GRID_COLS, shape)
    lines = tokens // GRID_COLS
    shape = (quarter, LANES)
    for first in range(0, lines, LANES):
        line = lax.broadcasted_iota(jnp.int32, shape, 1) + first + first_row
        cos_all, sin_all = pair(line, shape)
        half = lax.broadcasted_iota(jnp.int32, shape, 1) < GRID_COLS
        for r in range(0, min(LANES, lines - first), 2):
            cols = slice((first + r) * GRID_COLS, (first + r + 2) * GRID_COLS)
            for source, target in ((cos_all, cos_row), (sin_all, sin_row)):
                target[:, cols] = jnp.where(half, source[:, r : r + 1], source[:, r + 1 : r + 2])


def shards(
    latent,
    context,
    condition,
    ctx_cond,
    norm_gain,
    w_shift,
    w_scale,
    w_gate,
    w_query,
    w_key,
    w_value,
    w_out,
    sink_logit,
    ctx_lift,
):
    samples, tokens, width = latent.shape
    ctx_rows = context.shape[1]
    n_sp, n_tp, n_dp = lax.axis_size("sp"), lax.axis_size("tp"), lax.axis_size("dp")
    q_cols = w_query.shape[1]
    heads = q_cols // HEAD
    assert w_key.shape[1] == HEAD and tokens % GRID_COLS == 0 and samples < 4 and heads % 4 == 0 and n_tp == 4 and samples == 2
    part = w_shift.shape[1]
    block = tokens // n_tp
    ctx_all = n_sp * ctx_rows
    vmem = pl.BlockSpec(memory_space=pltpu.VMEM)
    anywhere = pl.BlockSpec(memory_space=pl.ANY)
    dma = pltpu.SemaphoreType.DMA
    padded = tokens + 2 * WINDOW
    proj = q_cols + 2 * HEAD
    keys = LANES + 2 * WINDOW + ctx_all
    V = pltpu.VMEM
    return pl.pallas_call(
        functools.partial(kernel, (n_sp, n_tp, n_dp)),
        out_shape=V((samples, block, width), bf16),
        in_specs=[anywhere] * 14,
        out_specs=vmem,
        scratch_shapes=[
            V(condition.shape, bf16),
            V(ctx_cond.shape, bf16),
            V((1, width), f32),
            pltpu.SMEM(sink_logit.shape, f32),
            pltpu.SMEM(ctx_lift.shape, f32),
            V(latent.shape, bf16),
            V(context.shape, bf16),
            V((3,) + w_shift.shape, bf16),
            V(w_query.shape, bf16),
            V((proj, width), bf16),
            V((samples, proj, width), bf16),
            V((2 * HEAD, width), bf16),
            V((HEAD // 4, tokens), f32),
            V((HEAD // 4, tokens), f32),
            V((HEAD // 4, block), f32),
            V((HEAD // 4, block), f32),
            V((n_tp,) + w_out.shape, bf16),
            V((8, w_shift.shape[0]), f32),
            V((n_sp, 4, 2 * part), f32),
            V((n_tp, 4, 2 * part), f32),
            V((n_sp, 4, part), f32),
            V((n_tp, 4, part), f32),
            V((8, width), f32),
            V((8, width), f32),
            V((8, width), f32),
            V((samples, 1, tokens), f32),
            V((samples, ctx_rows, LANES), f32),
            V((samples, proj, LANES), f32),
            V((8, 2 * HEAD), f32),
            V((samples, heads, LANES, tokens), bf16),
            V((samples, padded, LANES), bf16),
            V((samples, HEAD + ONES, padded), bf16),
            V((samples, ctx_all, LANES), bf16),
            V((samples, HEAD + ONES, ctx_all), bf16),
            V((2, WINDOW, LANES), f32),
            V((keys, 2 * LANES), f32),
            V((keys, 2 * LANES), f32),
            V((keys, 2 * LANES), f32),
            V((keys, 2 * LANES), f32),
            V((samples, n_tp, block, q_cols), bf16),
            V((n_tp, samples, block, q_cols), bf16),
            V((block, width), f32),
            dma((13 + samples,)),
            dma((n_sp,)),
            dma((n_sp,)),
            dma((n_tp,)),
            dma((n_tp,)),
            dma((n_sp,)),
            dma((n_sp,)),
            dma((n_tp,)),
            dma((n_tp,)),
            dma((samples, n_sp)),
            dma((samples, n_sp)),
            dma((samples, 2)),
            dma((samples, 2)),
            dma((samples, n_tp)),
            dma((samples, n_tp)),
            dma((3, PIECES)),
            dma((3, PIECES)),
            dma((3, n_dp)),
            dma((3, n_dp)),
        ],
        compiler_params=pltpu.CompilerParams(
            collective_id=0, has_side_effects=True, vmem_limit_bytes=56 * 1024 * 1024
        ),
    )(
        latent,
        context,
        condition,
        ctx_cond,
        norm_gain.reshape(1, -1),
        w_shift,
        w_scale,
        w_gate,
        w_query,
        w_key.T,
        w_value.T,
        w_out,
        sink_logit,
        ctx_lift,
    )


def solution(mesh):
    return jax.shard_map(
        shards,
        mesh=mesh,
        in_specs=(
            P("dp", "sp", None),
            P("dp", "sp", None),
            P("dp", "sp"),
            P("sp"),
            P(),
            P("sp", "tp"),
            P("sp", "tp"),
            P("sp", "tp"),
            P(None, "tp"),
            P(None, "tp"),
            P(None, "tp"),
            P("tp", None),
            P("tp"),
            P("tp"),
        ),
        out_specs=P("dp", ("sp", "tp"), None),
        check_vma=False,
    )
```

```python
import functools
import math

import jax
import jax.numpy as jnp
from jax import lax
from jax.experimental import pallas as pl
from jax.experimental.pallas import tpu as pltpu
from jax.sharding import PartitionSpec as P

HEAD = 64
WINDOW = 128
GRID_COLS = 64
LANES = 128
ONES = 16
PIECES = 8
EARLY = 2
AHEAD = 2

epsilon = 1e-06
rope_base = 10000.0
masked_value = -1e30
log2e = 1.4426950408889634
MESH = pl.DeviceIdType.MESH
nt = (((1,), (1,)), ((), ()))
f32 = jnp.float32
bf16 = jnp.bfloat16


def kernel(
    sizes,
    latent,
    context,
    condition_in,
    ctx_cond_in,
    norm_gain_in,
    w_shift,
    w_scale,
    w_gate,
    w_query,
    w_key,
    w_value,
    w_out,
    sink_logit_in,
    ctx_lift_in,
    out,
    condition,
    ctx_cond,
    norm_gain,
    sink_logit,
    ctx_lift,
    x_lat,
    x_ctx,
    w_mod,
    w_q,
    w_t,
    w_s,
    w_c,
    cos_row,
    sin_row,
    cos_col,
    sin_col,
    w_o,
    act,
    mod_rx,
    mod_all,
    gate_rx,
    gate_all,
    vec_a,
    vec_b,
    vec_g,
    inv_lat,
    inv_ctx,
    bias_col,
    bias_row,
    q_buf,
    kv_buf,
    vt_buf,
    ckv_buf,
    cvt_buf,
    mask_buf,
    s_a,
    s_b,
    s_c,
    s_d,
    att_buf,
    rows_rx,
    mix_buf,
    ld_sem,
    ma_send,
    ma_recv,
    mb_send,
    mb_recv,
    ga_send,
    ga_recv,
    gb_send,
    gb_recv,
    cx_send,
    cx_recv,
    ha_send,
    ha_recv,
    at_send,
    at_recv,
    wo_send,
    wo_recv,
    wf_send,
    wf_recv,
):
    n_sp, n_tp, n_dp = sizes
    me_sp, me_tp, me_dp = lax.axis_index("sp"), lax.axis_index("tp"), lax.axis_index("dp")
    samples, tokens, width = latent.shape
    ctx_rows = context.shape[1]
    ctx_all = n_sp * ctx_rows
    part = w_shift.shape[1]
    q_cols = w_query.shape[1]
    heads = q_cols // HEAD
    block = tokens // n_tp
    quarter = HEAD // 4
    q_scale = log2e * HEAD ** (-0.5)

    def other(me, step, count):
        return lax.rem(me + step, count)

    barrier = pltpu.get_barrier_semaphore()
    for axis, me, count in (("sp", me_sp, n_sp), ("tp", me_tp, n_tp), ("dp", me_dp, n_dp)):
        for step in range(1, count):
            pl.semaphore_signal(
                barrier, inc=1, device_id={axis: other(me, step, count)}, device_id_type=MESH
            )

    loads = []
    for source, target in (
        (condition_in, condition),
        (ctx_cond_in, ctx_cond),
        (w_shift, w_mod.at[0]),
        (w_scale, w_mod.at[1]),
        (context, x_ctx),
        (w_key, w_t.at[q_cols : q_cols + HEAD]),
        (w_value, w_t.at[q_cols + HEAD : q_cols + 2 * HEAD]),
        (w_query, w_q),
        (w_gate, w_mod.at[2]),
        *((latent.at[s], x_lat.at[s]) for s in range(samples)),
        (norm_gain_in, norm_gain),
        (sink_logit_in, sink_logit),
        (ctx_lift_in, ctx_lift),
        (w_out, w_o.at[me_tp]),
    ):
        copy = pltpu.make_async_copy(source, target, ld_sem.at[len(loads)])
        copy.start()
        loads.append(copy)

    def peers(axis, me, count, buffer, send, recv):
        def copy(step, source):
            return pltpu.make_async_remote_copy(
                src_ref=buffer.at[source],
                dst_ref=buffer.at[source],
                send_sem=send.at[step],
                recv_sem=recv.at[step],
                device_id={axis: other(me, step, count)},
                device_id_type=MESH,
            )

        def start():
            for step in range(1, count):
                copy(step, me).start()

        def arrive():
            for step in range(1, count):
                copy(step, other(me, count - step, count)).wait_recv()

        def finish():
            for step in range(1, count):
                copy(step, me).wait_send()

        return start, arrive, finish

    mod_a = peers("sp", me_sp, n_sp, mod_rx, ma_send, ma_recv)
    mod_b = peers("tp", me_tp, n_tp, mod_all, mb_send, mb_recv)
    gate_a = peers("sp", me_sp, n_sp, gate_rx, ga_send, ga_recv)
    gate_b = peers("tp", me_tp, n_tp, gate_all, gb_send, gb_recv)
    keep_rows = mod_rx.shape[1]

    share = w_out.shape[0] // n_dp
    piece = share // PIECES
    across = me_tp + 1 - 2 * lax.rem(me_tp, 2)
    along = lax.rem(me_tp + 2, n_tp)
    diagonal = lax.rem(across + 2, n_tp)

    def piece_copy(kind, i, source, target, local):
        rows = pl.ds(pl.multiple_of(me_dp * share + i * piece, piece), piece)
        return pltpu.make_async_remote_copy(
            src_ref=local.at[rows, :],
            dst_ref=w_o.at[source, rows, :],
            send_sem=wo_send.at[kind, i],
            recv_sem=wo_recv.at[kind, i],
            device_id={"tp": target},
            device_id_type=MESH,
        )

    own_order = (range(PIECES), [(i + PIECES // 2) % PIECES for i in range(PIECES)])

    def own_start(first, last):
        for i in range(first, last):
            for kind in range(2):
                own_copy(kind, own_order[kind][i]).start()

    def own_copy(kind, i):
        return piece_copy(kind, i, me_tp, (across, along)[kind], w_out)

    def relay_copy(i):
        source, target = ((across, along), (along, across))[2 * i // PIECES]
        return piece_copy(2, i, source, target, w_o.at[source])

    def piece_arrive(kind, i):
        source = (across, along, diagonal)[kind]
        target = (across, along, (along, across)[2 * i // PIECES])[kind]
        piece_copy(kind, i, source, target, w_o.at[source]).wait_recv()

    def relay():
        for i in range(PIECES // 2):
            for kind in range(2):
                piece_arrive(kind, own_order[kind][i])
                relay_copy(own_order[kind][i]).start()

    def forward_copy(source, index, hop, part_id):
        rows = pl.ds(pl.multiple_of(part_id * share, share), share)
        return pltpu.make_async_remote_copy(
            src_ref=w_o.at[source, rows, :],
            dst_ref=w_o.at[source, rows, :],
            send_sem=wf_send.at[index, hop],
            recv_sem=wf_recv.at[index, hop],
            device_id={"dp": other(me_dp, hop, n_dp)},
            device_id_type=MESH,
        )

    act[...] = jnp.zeros_like(act)
    loads[0].wait()
    loads[1].wait()
    cond = condition[...].astype(f32)
    act[0:samples, :] = cond / (1.0 + jnp.exp(-cond))
    cond = ctx_cond[...].astype(f32).reshape(1, -1)
    act[samples : samples + 1, :] = cond / (1.0 + jnp.exp(-cond))
    active = act[...].astype(bf16)
    for i in range(2):
        loads[2 + i].wait()
        mod_rx[me_sp, :, i * part : (i + 1) * part] = jnp.dot(
            active, w_mod[i], preferred_element_type=f32
        )[0:keep_rows].astype(bf16)
    pl.semaphore_wait(barrier, n_sp + n_tp + n_dp - 3)
    mod_a[0]()
    own_start(0, EARLY)

    loads[8].wait()
    gate_rx[me_sp] = jnp.dot(active, w_mod[2], preferred_element_type=f32)[0:keep_rows]
    gate_a[0]()

    loads[4].wait()
    for s in range(samples):
        wide = x_ctx[s].astype(f32)
        total = jnp.sum(wide * wide, axis=-1, keepdims=True)
        inv_ctx[s] = jnp.broadcast_to(lax.rsqrt(total / width + epsilon), (ctx_rows, LANES))

    loads[5].wait()
    loads[6].wait()
    loads[7].wait()
    for i in range(0, width, 256):
        w_t[0:q_cols, i : i + 256] = w_q[i : i + 256, :].T

    fill_tables(me_sp * (tokens // GRID_COLS), cos_row, sin_row, cos_col, sin_col)
    key_id = lax.broadcasted_iota(jnp.int32, (WINDOW, LANES), 0)
    query_id = lax.broadcasted_iota(jnp.int32, (WINDOW, LANES), 1)
    mask_buf[0] = jnp.where(key_id >= query_id, 0.0, masked_value)
    mask_buf[1] = jnp.where(key_id <= query_id, 0.0, masked_value)
    q_buf[:, :, HEAD:, :] = jnp.zeros(q_buf.shape[:2] + (LANES - HEAD, tokens), bf16)
    vt_buf[:, HEAD:, :] = jnp.ones((samples, ONES, vt_buf.shape[2]), bf16)
    cvt_buf[:, HEAD:, :] = jnp.ones((samples, ONES, ctx_all), bf16)
    vec_b[...] = jnp.zeros_like(vec_b)

    def stats(s):
        def body(i, carry):
            rows = pl.ds(pl.multiple_of(i * block, block), block)
            wide = x_lat[s, rows, :].astype(f32)
            acc = wide[:, 0:LANES] * wide[:, 0:LANES]
            for k in range(LANES, width, LANES):
                acc = acc + wide[:, k : k + LANES] * wide[:, k : k + LANES]
            total = jnp.sum(acc.T, axis=0, keepdims=True)
            inv_lat[s, :, rows] = lax.rsqrt(total / width + epsilon)
            return carry

        lax.fori_loop(0, n_tp, body, 0)

    loads[9].wait()
    stats(0)

    mod_a[1]()
    total = mod_rx[0].astype(f32)
    for i in range(1, n_sp):
        total = total + mod_rx[i].astype(f32)
    mod_all[me_tp] = total.astype(bf16)
    mod_b[0]()
    own_start(EARLY, PIECES)

    for s in range(1, samples):
        loads[9 + s].wait()
        stats(s)

    gate_a[1]()
    total = gate_rx[0]
    for i in range(1, n_sp):
        total = total + gate_rx[i]
    gate_all[me_tp] = total
    gate_b[0]()

    for i in range(2, 5):
        loads[-i].wait()

    mod_b[1]()
    for t in range(n_tp):
        cols = slice(t * part, (t + 1) * part)
        vec_b[0:keep_rows, cols] = mod_all[t, :, 0:part].astype(f32)
        vec_a[0:keep_rows, cols] = (1.0 + mod_all[t, :, part : 2 * part].astype(f32)) * norm_gain[:, cols]

    def fold(target, first, last, base, row):
        gain = vec_a[row : row + 1, :]
        for r in range(first, last, 32):
            target[r - base : r - base + 32, :] = (w_t[r : r + 32, :].astype(f32) * gain).astype(bf16)

    shift = vec_b[...]
    high = shift.astype(bf16).astype(f32)
    shift_pair = jnp.concatenate([high, shift - high], axis=0).astype(bf16)
    bias = lax.dot_general(shift_pair, w_t[q_cols:, :], nt, preferred_element_type=f32)
    bias_row[...] = bias[0:8] + bias[8:16]
    fold(w_c, q_cols, q_cols + 2 * HEAD, q_cols, samples)

    def ctx_copy(s, step, source):
        rows = pl.ds(pl.multiple_of(source * ctx_rows, ctx_rows), ctx_rows)
        return pltpu.make_async_remote_copy(
            src_ref=ckv_buf.at[s, rows, :],
            dst_ref=ckv_buf.at[s, rows, :],
            send_sem=cx_send.at[s, step],
            recv_sem=cx_recv.at[s, step],
            device_id={"sp": other(me_sp, step, n_sp)},
            device_id_type=MESH,
        )

    def context_keys(s):
        rows = pl.ds(pl.multiple_of(me_sp * ctx_rows, ctx_rows), ctx_rows)
        kv = lax.dot_general(x_ctx[s], w_c[...], nt, preferred_element_type=f32)
        ckv_buf[s, rows, :] = (kv * inv_ctx[s] + bias_row[samples : samples + 1, :]).astype(bf16)
        for far in range(n_sp - 1, 0, -1):

            @pl.when(me_sp + far < n_sp)
            def _():
                ctx_copy(s, far, me_sp).start()

            @pl.when(me_sp >= far)
            def _():
                ctx_copy(s, n_sp - far, me_sp).start()

    context_keys(0)

    def fold_sample(s):
        fold(w_s.at[s], 0, q_cols + 2 * HEAD, 0, s)
        bias_col[s, 0:q_cols, :] = jnp.broadcast_to(column[0:q_cols, s : s + 1] * q_scale, (q_cols, LANES))
        bias_col[s, q_cols:, :] = jnp.broadcast_to(column[q_cols:, s : s + 1], (2 * HEAD, LANES))

    bias = lax.dot_general(shift_pair, w_t[0:q_cols, :], nt, preferred_element_type=f32)
    bias = jnp.concatenate([bias[0:8] + bias[8:16], bias_row[...]], axis=1)
    bias = jnp.concatenate([bias, jnp.zeros((LANES - 8, bias.shape[1]), f32)], axis=0)
    column = bias.T

    def halo_copy(s, side):
        source, target = ((tokens, 0), (WINDOW, WINDOW + tokens))[side]
        step = (1, n_sp - 1)[side]
        return pltpu.make_async_remote_copy(
            src_ref=kv_buf.at[s, pl.ds(source, WINDOW), :],
            dst_ref=kv_buf.at[s, pl.ds(target, WINDOW), :],
            send_sem=ha_send.at[s, side],
            recv_sem=ha_recv.at[s, side],
            device_id={"sp": other(me_sp, step, n_sp)},
            device_id_type=MESH,
        )

    has_left, has_right = me_sp > 0, me_sp < n_sp - 1

    def halo_sends(s, act_on):
        for side, present in ((0, has_right), (1, has_left)):

            @pl.when(present)
            def _():
                act_on(halo_copy(s, side))

    def project(s, start):
        cols = slice(start, start + block)
        y = lax.dot_general(w_s[s], x_lat[s, cols, :], nt, preferred_element_type=f32)
        inv = inv_lat[s, :, cols]
        inv_q = inv * q_scale
        cr, sr = cos_row[:, cols], sin_row[:, cols]
        cc, sc = cos_col[...], sin_col[...]

        def wide(first, count):
            return jnp.concatenate([bias_col[s, first : first + count, :]] * (block // LANES), axis=1)

        def rotated(base, scale):
            u = [
                y[base + k * quarter : base + (k + 1) * quarter] * scale
                + wide(base + k * quarter, quarter)
                for k in range(4)
            ]
            return (
                u[0] * cr - u[1] * sr,
                u[0] * sr + u[1] * cr,
                u[2] * cc - u[3] * sc,
                u[2] * sc + u[3] * cc,
            )

        for h in range(heads):
            q_buf[s, h, 0:HEAD, cols] = jnp.concatenate(rotated(h * HEAD, inv_q), axis=0).astype(bf16)
        v = y[q_cols + HEAD :] * inv + wide(q_cols + HEAD, HEAD)
        kv = jnp.concatenate((*rotated(q_cols, inv), v), axis=0)
        vt_buf[s, 0:HEAD, WINDOW + start : WINDOW + start + block] = v.astype(bf16)
        kv_buf[s, WINDOW + start : WINDOW + start + block, :] = kv.T.astype(bf16)

    for s in range(samples):
        fold_sample(s)
        project(s, 0)
        project(s, tokens - block)
        halo_sends(s, lambda copy: copy.start())
        for i in range(1, n_tp - 1):
            project(s, i * block)
        if s > 0:
            context_keys(s)
        if s == 0:
            relay()

    halves = block // LANES

    def rows_copy(s, step, source):
        target = other(me_tp, step, n_tp)
        return pltpu.make_async_remote_copy(
            src_ref=att_buf.at[s, target],
            dst_ref=rows_rx.at[source, s],
            send_sem=at_send.at[s, step],
            recv_sem=at_recv.at[s, step],
            device_id={"tp": target},
            device_id_type=MESH,
        )

    pairs = heads // 2
    near_rows = LANES + 2 * WINDOW
    low = lax.broadcasted_iota(jnp.int32, (1, 2 * LANES), 1) < LANES

    def two(ref, pair):
        return jnp.where(low, ref[2 * pair], ref[2 * pair + 1]) * log2e

    def start_of(index):
        step = index // halves + 1
        owner = other(me_tp, step, n_tp)
        return pl.multiple_of(owner * block + (index % halves) * LANES, LANES)

    def chunks_of(near, far):
        return [(False, c, min(near, near_rows - c)) for c in range(0, near_rows, near)] + [
            (True, c, min(far, ctx_all)) for c in range(0, ctx_all, min(far, ctx_all))
        ]

    score_chunks = chunks_of(384, 256)
    value_chunks = chunks_of(256, 256)

    def score_steps(s, index, pair, buf, state):
        start = start_of(index)
        cols = pl.ds(start, LANES)
        q = jnp.concatenate(
            [q_buf[s, 2 * pair, :, cols], q_buf[s, 2 * pair + 1, :, cols]], axis=1
        )
        tops = [None, None]

        def one(chunk):
            far, first, count = chunk
            if far:
                keys = ckv_buf[s, first : first + count, :]
            else:
                keys = kv_buf[s, pl.ds(start + first, count), :]
            scores = jnp.dot(keys, q, preferred_element_type=f32)
            base = near_rows + first if far else first
            if not far:
                parts = [scores[r : r + WINDOW] for r in range(0, count, WINDOW)]
                for edge, place in ((0, 0), (1, near_rows - WINDOW)):
                    if first <= place < first + count:
                        mask = jnp.concatenate([mask_buf[edge], mask_buf[edge]], axis=1)
                        parts[(place - first) // WINDOW] += mask
                scores = jnp.concatenate(parts, axis=0)
            buf[base : base + count, :] = scores
            high = jnp.max(scores.reshape(count // 8, 8, 2 * LANES), axis=0)
            tops[far] = high if tops[far] is None else jnp.maximum(tops[far], high)

        for chunk in score_chunks:
            yield functools.partial(one, chunk)

        def close():
            near_top = jnp.max(tops[0], axis=0, keepdims=True)
            far_top = jnp.max(tops[1], axis=0, keepdims=True)
            lift = two(ctx_lift, pair)
            state.append(
                jnp.maximum(jnp.maximum(near_top, far_top + lift), two(sink_logit, pair))
            )

        yield close

    def value_steps(s, index, pair, buf, top):
        start = start_of(index)
        far_top = top - two(ctx_lift, pair)
        acc = [None]

        def one(chunk):
            far, first, count = chunk
            base = near_rows + first if far else first
            p = jnp.exp2(buf[base : base + count, :] - (far_top if far else top)).astype(bf16)
            if far:
                values = cvt_buf[s, :, first : first + count]
            else:
                values = vt_buf[s, :, pl.ds(start + first, count)]
            term = jnp.dot(values, p, preferred_element_type=f32)
            acc[0] = term if acc[0] is None else acc[0] + term

        for chunk in value_chunks:
            yield functools.partial(one, chunk)

        def close():
            weight = acc[0][HEAD : HEAD + 1] + jnp.exp2(two(sink_logit, pair) - top)
            rows = acc[0][0:HEAD] * (1.0 / weight)
            stacked = jnp.concatenate([rows[:, 0:LANES], rows[:, LANES:]], axis=0)
            owner = other(me_tp, index // halves + 1, n_tp)
            half = pl.multiple_of((index % halves) * LANES, LANES)
            att_buf[s, owner, pl.ds(half, LANES), pair * LANES : (pair + 1) * LANES] = (
                stacked.T.astype(bf16)
            )

        yield close

    def run(*streams):
        streams = [list(steps) for steps in streams]
        order = sorted(
            ((i + 1) / len(steps), k, i) for k, steps in enumerate(streams) for i in range(len(steps))
        )
        for _, k, i in order:
            streams[k][i]()

    bufs = (s_a, s_b, s_c, s_d)
    per_step = halves * pairs

    def forward(kinds):
        for index in kinds:
            source = (across, along, diagonal)[index]
            for i in range(PIECES):
                if index == 2 or 2 * i // PIECES != index:
                    piece_arrive(index, i)
            for hop in range(1, n_dp):
                forward_copy(source, index, hop, me_dp).start()

    def attention(s):
        def scores_of(unit, base, target):
            return score_steps(s, base + unit // pairs, unit % pairs, bufs[unit % len(bufs)], target)

        tops = [[] for _ in range(AHEAD)]
        run(*(scores_of(unit, 0, tops[unit]) for unit in range(AHEAD)))

        def body(step, tops, last):
            base = step * halves
            known = [[top] for top in tops]
            for unit in range(per_step):
                streams = []
                if not last or unit + AHEAD < per_step:
                    known.append([])
                    streams.append(scores_of(unit + AHEAD, base, known[-1]))
                streams.append(
                    value_steps(
                        s, base + unit // pairs, unit % pairs, bufs[unit % len(bufs)], known[unit][0]
                    )
                )
                run(*streams)
            if not last:
                rows_copy(s, step + 1, me_tp).start()
                if s == samples - 1:
                    pl.when(step == 0)(lambda: forward((2,)))
            return tuple(top[0] for top in known[per_step:])

        tops = tuple(top[0] for top in tops)
        tops = lax.fori_loop(0, n_tp - 1, lambda step, tops: body(step, tops, False), tops)
        body(n_tp - 1, tops, True)
        rows_rx[me_tp, s] = att_buf[s, me_tp]

    def context_ready(s):
        for step in range(1, n_sp):
            ctx_copy(s, step, other(me_sp, n_sp - step, n_sp)).wait_recv()
        for c in range(0, ctx_all, 256):
            cvt_buf[s, 0:HEAD, c : c + 256] = ckv_buf[s, c : c + 256, :].T[HEAD:]

    def halo_ready(s):
        for side in range(2):
            first = (0, WINDOW + tokens)[side]
            valid = (has_left, has_right)[side]
            halo = slice(first, first + WINDOW)

            @pl.when(valid)
            def _():
                halo_copy(s, side).wait_recv()

            @pl.when(jnp.logical_not(valid))
            def _():
                kv_buf[s, halo, :] = jnp.zeros((WINDOW, LANES), bf16)
                vt_buf[s, HEAD:, halo] = jnp.zeros((ONES, WINDOW), bf16)

            vt_buf[s, 0:HEAD, halo] = kv_buf[s, halo, :].T[HEAD:]

    for s in range(samples):
        halo_ready(s)
        context_ready(s)
        attention(s)
        if s == 0:
            forward((0, 1))

    gate_b[1]()
    for t in range(n_tp):
        vec_g[0:keep_rows, t * part : (t + 1) * part] = gate_all[t]

    loads[-1].wait()
    for index, source in enumerate((across, along, diagonal)):
        for hop in range(1, n_dp):
            forward_copy(source, index, hop, other(me_dp, n_dp - hop, n_dp)).wait_recv()
    chunk = 512

    def rows_arrive(s, step):
        rows_copy(s, step, other(me_tp, n_tp - step, n_tp)).wait_recv()

    def mix(s, steps, c):
        acc = None
        for step in steps:
            t = other(me_tp, n_tp - step, n_tp)
            term = jnp.dot(rows_rx[t, s], w_o[t, :, c : c + chunk], preferred_element_type=f32)
            acc = term if acc is None else acc + term
        return acc

    for s in range(samples):
        final = s == samples - 1
        for step in range(1, n_tp - 1 if final else n_tp):
            rows_arrive(s, step)
        for c in range(0, width, chunk):
            cols = slice(c, c + chunk)
            if final:
                mix_buf[:, cols] = mix(s, range(n_tp - 1), c)
            else:
                out[s, :, cols] = (mix(s, range(n_tp), c) * vec_g[s : s + 1, cols]).astype(bf16)
    rows_arrive(samples - 1, n_tp - 1)
    for c in range(0, width, chunk):
        cols = slice(c, c + chunk)
        acc = mix_buf[:, cols] + mix(samples - 1, (n_tp - 1,), c)
        out[samples - 1, :, cols] = (acc * vec_g[samples - 1 : samples, cols]).astype(bf16)

    for _, _, finish_send in (mod_a, mod_b, gate_a, gate_b):
        finish_send()
    for s in range(samples):
        for step in range(1, n_sp):
            ctx_copy(s, step, me_sp).wait_send()
        halo_sends(s, lambda copy: copy.wait_send())
    for i in range(PIECES):
        own_copy(0, i).wait_send()
        own_copy(1, i).wait_send()
        relay_copy(i).wait_send()
    for index, source in enumerate((across, along, diagonal)):
        for hop in range(1, n_dp):
            forward_copy(source, index, hop, me_dp).wait_send()
    for step in range(1, n_tp):
        for s in range(samples):
            rows_copy(s, step, me_tp).wait_send()


def fill_tables(first_row, cos_row, sin_row, cos_col, sin_col):
    tokens = cos_row.shape[1]
    quarter = HEAD // 4

    def pair(ticks, shape):
        power = lax.broadcasted_iota(jnp.int32, shape, 0).astype(f32)
        angles = ticks.astype(f32) * jnp.exp(power * (-math.log(rope_base) / quarter))
        return jnp.cos(angles), jnp.sin(angles)

    shape = cos_col.shape
    token = lax.broadcasted_iota(jnp.int32, shape, 1)
    cos_col[...], sin_col[...] = pair(token % GRID_COLS, shape)
    lines = tokens // GRID_COLS
    shape = (quarter, LANES)
    for first in range(0, lines, LANES):
        line = lax.broadcasted_iota(jnp.int32, shape, 1) + first + first_row
        cos_all, sin_all = pair(line, shape)
        half = lax.broadcasted_iota(jnp.int32, shape, 1) < GRID_COLS
        for r in range(0, min(LANES, lines - first), 2):
            cols = slice((first + r) * GRID_COLS, (first + r + 2) * GRID_COLS)
            for source, target in ((cos_all, cos_row), (sin_all, sin_row)):
                target[:, cols] = jnp.where(half, source[:, r : r + 1], source[:, r + 1 : r + 2])


def shards(
    latent,
    context,
    condition,
    ctx_cond,
    norm_gain,
    w_shift,
    w_scale,
    w_gate,
    w_query,
    w_key,
    w_value,
    w_out,
    sink_logit,
    ctx_lift,
):
    samples, tokens, width = latent.shape
    ctx_rows = context.shape[1]
    n_sp, n_tp, n_dp = lax.axis_size("sp"), lax.axis_size("tp"), lax.axis_size("dp")
    q_cols = w_query.shape[1]
    heads = q_cols // HEAD
    assert w_key.shape[1] == HEAD and tokens % GRID_COLS == 0 and samples < 4 and heads % 4 == 0 and n_tp == 4 and samples == 2
    part = w_shift.shape[1]
    block = tokens // n_tp
    ctx_all = n_sp * ctx_rows
    vmem = pl.BlockSpec(memory_space=pltpu.VMEM)
    anywhere = pl.BlockSpec(memory_space=pl.ANY)
    dma = pltpu.SemaphoreType.DMA
    padded = tokens + 2 * WINDOW
    proj = q_cols + 2 * HEAD
    keys = LANES + 2 * WINDOW + ctx_all
    V = pltpu.VMEM
    return pl.pallas_call(
        functools.partial(kernel, (n_sp, n_tp, n_dp)),
        out_shape=V((samples, block, width), bf16),
        in_specs=[anywhere] * 14,
        out_specs=vmem,
        scratch_shapes=[
            V(condition.shape, bf16),
            V(ctx_cond.shape, bf16),
            V((1, width), f32),
            pltpu.SMEM(sink_logit.shape, f32),
            pltpu.SMEM(ctx_lift.shape, f32),
            V(latent.shape, bf16),
            V(context.shape, bf16),
            V((3,) + w_shift.shape, bf16),
            V(w_query.shape, bf16),
            V((proj, width), bf16),
            V((samples, proj, width), bf16),
            V((2 * HEAD, width), bf16),
            V((HEAD // 4, tokens), f32),
            V((HEAD // 4, tokens), f32),
            V((HEAD // 4, block), f32),
            V((HEAD // 4, block), f32),
            V((n_tp,) + w_out.shape, bf16),
            V((8, w_shift.shape[0]), f32),
            V((n_sp, 4, 2 * part), bf16),
            V((n_tp, 4, 2 * part), bf16),
            V((n_sp, 4, part), f32),
            V((n_tp, 4, part), f32),
            V((8, width), f32),
            V((8, width), f32),
            V((8, width), f32),
            V((samples, 1, tokens), f32),
            V((samples, ctx_rows, LANES), f32),
            V((samples, proj, LANES), f32),
            V((8, 2 * HEAD), f32),
            V((samples, heads, LANES, tokens), bf16),
            V((samples, padded, LANES), bf16),
            V((samples, HEAD + ONES, padded), bf16),
            V((samples, ctx_all, LANES), bf16),
            V((samples, HEAD + ONES, ctx_all), bf16),
            V((2, WINDOW, LANES), f32),
            V((keys, 2 * LANES), f32),
            V((keys, 2 * LANES), f32),
            V((keys, 2 * LANES), f32),
            V((keys, 2 * LANES), f32),
            V((samples, n_tp, block, q_cols), bf16),
            V((n_tp, samples, block, q_cols), bf16),
            V((block, width), f32),
            dma((13 + samples,)),
            dma((n_sp,)),
            dma((n_sp,)),
            dma((n_tp,)),
            dma((n_tp,)),
            dma((n_sp,)),
            dma((n_sp,)),
            dma((n_tp,)),
            dma((n_tp,)),
            dma((samples, n_sp)),
            dma((samples, n_sp)),
            dma((samples, 2)),
            dma((samples, 2)),
            dma((samples, n_tp)),
            dma((samples, n_tp)),
            dma((3, PIECES)),
            dma((3, PIECES)),
            dma((3, n_dp)),
            dma((3, n_dp)),
        ],
        compiler_params=pltpu.CompilerParams(
            collective_id=0, has_side_effects=True, vmem_limit_bytes=56 * 1024 * 1024
        ),
    )(
        latent,
        context,
        condition,
        ctx_cond,
        norm_gain.reshape(1, -1),
        w_shift,
        w_scale,
        w_gate,
        w_query,
        w_key.T,
        w_value.T,
        w_out,
        sink_logit,
        ctx_lift,
    )


def solution(mesh):
    return jax.shard_map(
        shards,
        mesh=mesh,
        in_specs=(
            P("dp", "sp", None),
            P("dp", "sp", None),
            P("dp", "sp"),
            P("sp"),
            P(),
            P("sp", "tp"),
            P("sp", "tp"),
            P("sp", "tp"),
            P(None, "tp"),
            P(None, "tp"),
            P(None, "tp"),
            P("tp", None),
            P("tp"),
            P("tp"),
        ),
        out_specs=P("dp", ("sp", "tp"), None),
        check_vma=False,
    )
```

```python
import functools
import math

import jax
import jax.numpy as jnp
from jax import lax
from jax.experimental import pallas as pl
from jax.experimental.pallas import tpu as pltpu
from jax.sharding import PartitionSpec as P

HEAD = 64
WINDOW = 128
GRID_COLS = 64
LANES = 128
ONES = 16
PIECES = 8
EARLY = 2
AHEAD = 2

epsilon = 1e-06
rope_base = 10000.0
masked_value = -1e30
log2e = 1.4426950408889634
MESH = pl.DeviceIdType.MESH
nt = (((1,), (1,)), ((), ()))
f32 = jnp.float32
bf16 = jnp.bfloat16


def kernel(
    sizes,
    latent,
    context,
    condition_in,
    ctx_cond_in,
    norm_gain_in,
    w_shift,
    w_scale,
    w_gate,
    w_query,
    w_key,
    w_value,
    w_out,
    sink_logit_in,
    ctx_lift_in,
    out,
    condition,
    ctx_cond,
    norm_gain,
    sink_logit,
    ctx_lift,
    x_lat,
    x_ctx,
    w_mod,
    w_q,
    w_t,
    w_s,
    w_c,
    cos_row,
    sin_row,
    cos_col,
    sin_col,
    w_o,
    act,
    mod_rx,
    mod_all,
    gate_rx,
    gate_all,
    vec_a,
    vec_b,
    vec_g,
    inv_lat,
    inv_ctx,
    bias_col,
    bias_row,
    q_buf,
    kv_buf,
    vt_buf,
    ckv_buf,
    cvt_buf,
    mask_buf,
    s_a,
    s_b,
    s_c,
    s_d,
    att_buf,
    rows_rx,
    mix_buf,
    ld_sem,
    ma_send,
    ma_recv,
    mb_send,
    mb_recv,
    ga_send,
    ga_recv,
    gb_send,
    gb_recv,
    cx_send,
    cx_recv,
    ha_send,
    ha_recv,
    at_send,
    at_recv,
    wo_send,
    wo_recv,
    wf_send,
    wf_recv,
):
    n_sp, n_tp, n_dp = sizes
    me_sp, me_tp, me_dp = lax.axis_index("sp"), lax.axis_index("tp"), lax.axis_index("dp")
    samples, tokens, width = latent.shape
    ctx_rows = context.shape[1]
    ctx_all = n_sp * ctx_rows
    part = w_shift.shape[1]
    q_cols = w_query.shape[1]
    heads = q_cols // HEAD
    block = tokens // n_tp
    quarter = HEAD // 4
    q_scale = log2e * HEAD ** (-0.5)

    def other(me, step, count):
        return lax.rem(me + step, count)

    barrier = pltpu.get_barrier_semaphore()
    for axis, me, count in (("sp", me_sp, n_sp), ("tp", me_tp, n_tp), ("dp", me_dp, n_dp)):
        for step in range(1, count):
            pl.semaphore_signal(
                barrier, inc=1, device_id={axis: other(me, step, count)}, device_id_type=MESH
            )

    loads = []
    for source, target in (
        (condition_in, condition),
        (ctx_cond_in, ctx_cond),
        (w_shift, w_mod.at[0]),
        (w_scale, w_mod.at[1]),
        (context, x_ctx),
        (w_key, w_t.at[q_cols : q_cols + HEAD]),
        (w_value, w_t.at[q_cols + HEAD : q_cols + 2 * HEAD]),
        (w_query, w_q),
        (w_gate, w_mod.at[2]),
        *((latent.at[s], x_lat.at[s]) for s in range(samples)),
        (norm_gain_in, norm_gain),
        (sink_logit_in, sink_logit),
        (ctx_lift_in, ctx_lift),
        (w_out, w_o.at[me_tp]),
    ):
        copy = pltpu.make_async_copy(source, target, ld_sem.at[len(loads)])
        copy.start()
        loads.append(copy)

    def peers(axis, me, count, buffer, send, recv):
        def copy(step, source):
            return pltpu.make_async_remote_copy(
                src_ref=buffer.at[source],
                dst_ref=buffer.at[source],
                send_sem=send.at[step],
                recv_sem=recv.at[step],
                device_id={axis: other(me, step, count)},
                device_id_type=MESH,
            )

        def start():
            for step in range(1, count):
                copy(step, me).start()

        def arrive():
            for step in range(1, count):
                copy(step, other(me, count - step, count)).wait_recv()

        def finish():
            for step in range(1, count):
                copy(step, me).wait_send()

        return start, arrive, finish

    mod_a = peers("sp", me_sp, n_sp, mod_rx, ma_send, ma_recv)
    mod_b = peers("tp", me_tp, n_tp, mod_all, mb_send, mb_recv)
    gate_a = peers("sp", me_sp, n_sp, gate_rx, ga_send, ga_recv)
    gate_b = peers("tp", me_tp, n_tp, gate_all, gb_send, gb_recv)
    keep_rows = mod_rx.shape[1]

    share = w_out.shape[0] // n_dp
    piece = share // PIECES
    across = me_tp + 1 - 2 * lax.rem(me_tp, 2)
    along = lax.rem(me_tp + 2, n_tp)
    diagonal = lax.rem(across + 2, n_tp)

    def piece_copy(kind, i, source, target, local):
        rows = pl.ds(pl.multiple_of(me_dp * share + i * piece, piece), piece)
        return pltpu.make_async_remote_copy(
            src_ref=local.at[rows, :],
            dst_ref=w_o.at[source, rows, :],
            send_sem=wo_send.at[kind, i],
            recv_sem=wo_recv.at[kind, i],
            device_id={"tp": target},
            device_id_type=MESH,
        )

    own_order = (range(PIECES), [(i + PIECES // 2) % PIECES for i in range(PIECES)])

    def own_start(first, last):
        for i in range(first, last):
            for kind in range(2):
                own_copy(kind, own_order[kind][i]).start()

    def own_copy(kind, i):
        return piece_copy(kind, i, me_tp, (across, along)[kind], w_out)

    def relay_copy(i):
        source, target = ((across, along), (along, across))[2 * i // PIECES]
        return piece_copy(2, i, source, target, w_o.at[source])

    def piece_arrive(kind, i):
        source = (across, along, diagonal)[kind]
        target = (across, along, (along, across)[2 * i // PIECES])[kind]
        piece_copy(kind, i, source, target, w_o.at[source]).wait_recv()

    def relay():
        for i in range(PIECES // 2):
            for kind in range(2):
                piece_arrive(kind, own_order[kind][i])
                relay_copy(own_order[kind][i]).start()

    def forward_copy(source, index, hop, part_id):
        rows = pl.ds(pl.multiple_of(part_id * share, share), share)
        return pltpu.make_async_remote_copy(
            src_ref=w_o.at[source, rows, :],
            dst_ref=w_o.at[source, rows, :],
            send_sem=wf_send.at[index, hop],
            recv_sem=wf_recv.at[index, hop],
            device_id={"dp": other(me_dp, hop, n_dp)},
            device_id_type=MESH,
        )

    act[...] = jnp.zeros_like(act)
    loads[0].wait()
    loads[1].wait()
    cond = condition[...].astype(f32)
    act[0:samples, :] = cond / (1.0 + jnp.exp(-cond))
    cond = ctx_cond[...].astype(f32).reshape(1, -1)
    act[samples : samples + 1, :] = cond / (1.0 + jnp.exp(-cond))
    active = act[...].astype(bf16)
    for i in range(2):
        loads[2 + i].wait()
        mod_rx[me_sp, :, i * part : (i + 1) * part] = jnp.dot(
            active, w_mod[i], preferred_element_type=f32
        )[0:keep_rows].astype(bf16)
    pl.semaphore_wait(barrier, n_sp + n_tp + n_dp - 3)
    mod_a[0]()
    own_start(0, EARLY)

    loads[8].wait()
    gate_rx[me_sp] = jnp.dot(active, w_mod[2], preferred_element_type=f32)[0:keep_rows]
    gate_a[0]()

    loads[4].wait()
    for s in range(samples):
        wide = x_ctx[s].astype(f32)
        total = jnp.sum(wide * wide, axis=-1, keepdims=True)
        inv_ctx[s] = jnp.broadcast_to(lax.rsqrt(total / width + epsilon), (ctx_rows, LANES))

    loads[5].wait()
    loads[6].wait()
    loads[7].wait()
    for i in range(0, width, 256):
        w_t[0:q_cols, i : i + 256] = w_q[i : i + 256, :].T

    fill_tables(me_sp * (tokens // GRID_COLS), cos_row, sin_row, cos_col, sin_col)
    key_id = lax.broadcasted_iota(jnp.int32, (WINDOW, LANES), 0)
    query_id = lax.broadcasted_iota(jnp.int32, (WINDOW, LANES), 1)
    mask_buf[0] = jnp.where(key_id >= query_id, 0.0, masked_value)
    mask_buf[1] = jnp.where(key_id <= query_id, 0.0, masked_value)
    q_buf[:, :, HEAD:, :] = jnp.zeros(q_buf.shape[:2] + (LANES - HEAD, tokens), bf16)
    vt_buf[:, HEAD:, :] = jnp.ones((samples, ONES, vt_buf.shape[2]), bf16)
    cvt_buf[:, HEAD:, :] = jnp.ones((samples, ONES, ctx_all), bf16)
    vec_b[...] = jnp.zeros_like(vec_b)

    def stats(s):
        def body(i, carry):
            rows = pl.ds(pl.multiple_of(i * block, block), block)
            wide = x_lat[s, rows, :].astype(f32)
            acc = wide[:, 0:LANES] * wide[:, 0:LANES]
            for k in range(LANES, width, LANES):
                acc = acc + wide[:, k : k + LANES] * wide[:, k : k + LANES]
            total = jnp.sum(acc.T, axis=0, keepdims=True)
            inv_lat[s, :, rows] = lax.rsqrt(total / width + epsilon)
            return carry

        lax.fori_loop(0, n_tp, body, 0)

    loads[9].wait()
    stats(0)

    mod_a[1]()
    total = mod_rx[0].astype(f32)
    for i in range(1, n_sp):
        total = total + mod_rx[i].astype(f32)
    mod_all[me_tp] = total.astype(bf16)
    mod_b[0]()
    own_start(EARLY, PIECES)

    for s in range(1, samples):
        loads[9 + s].wait()
        stats(s)

    gate_a[1]()
    total = gate_rx[0]
    for i in range(1, n_sp):
        total = total + gate_rx[i]
    gate_all[me_tp] = total
    gate_b[0]()

    for i in range(2, 5):
        loads[-i].wait()

    mod_b[1]()
    for t in range(n_tp):
        cols = slice(t * part, (t + 1) * part)
        vec_b[0:keep_rows, cols] = mod_all[t, :, 0:part].astype(f32)
        vec_a[0:keep_rows, cols] = (1.0 + mod_all[t, :, part : 2 * part].astype(f32)) * norm_gain[:, cols]

    def fold(target, first, last, base, row):
        gain = vec_a[row : row + 1, :]
        for r in range(first, last, 32):
            target[r - base : r - base + 32, :] = (w_t[r : r + 32, :].astype(f32) * gain).astype(bf16)

    shift = vec_b[...]
    high = shift.astype(bf16).astype(f32)
    shift_pair = jnp.concatenate([high, shift - high], axis=0).astype(bf16)
    bias = lax.dot_general(shift_pair, w_t[q_cols:, :], nt, preferred_element_type=f32)
    bias_row[...] = bias[0:8] + bias[8:16]
    fold(w_c, q_cols, q_cols + 2 * HEAD, q_cols, samples)

    def ctx_copy(s, step, source):
        rows = pl.ds(pl.multiple_of(source * ctx_rows, ctx_rows), ctx_rows)
        return pltpu.make_async_remote_copy(
            src_ref=ckv_buf.at[s, rows, :],
            dst_ref=ckv_buf.at[s, rows, :],
            send_sem=cx_send.at[s, step],
            recv_sem=cx_recv.at[s, step],
            device_id={"sp": other(me_sp, step, n_sp)},
            device_id_type=MESH,
        )

    def context_keys(s):
        rows = pl.ds(pl.multiple_of(me_sp * ctx_rows, ctx_rows), ctx_rows)
        kv = lax.dot_general(x_ctx[s], w_c[...], nt, preferred_element_type=f32)
        ckv_buf[s, rows, :] = (kv * inv_ctx[s] + bias_row[samples : samples + 1, :]).astype(bf16)

    def context_sends(s, turn):
        for far in range(n_sp - 1, 0, -1):

            @pl.when(turn & (me_sp + far < n_sp))
            def _():
                ctx_copy(s, far, me_sp).start()

            @pl.when(turn & (me_sp >= far))
            def _():
                ctx_copy(s, n_sp - far, me_sp).start()

    first_turn = me_dp < n_dp - 1
    context_keys(0)
    context_sends(0, me_sp >= 0)

    def fold_sample(s):
        fold(w_s.at[s], 0, q_cols + 2 * HEAD, 0, s)
        bias_col[s, 0:q_cols, :] = jnp.broadcast_to(column[0:q_cols, s : s + 1] * q_scale, (q_cols, LANES))
        bias_col[s, q_cols:, :] = jnp.broadcast_to(column[q_cols:, s : s + 1], (2 * HEAD, LANES))

    bias = lax.dot_general(shift_pair, w_t[0:q_cols, :], nt, preferred_element_type=f32)
    bias = jnp.concatenate([bias[0:8] + bias[8:16], bias_row[...]], axis=1)
    bias = jnp.concatenate([bias, jnp.zeros((LANES - 8, bias.shape[1]), f32)], axis=0)
    column = bias.T

    def halo_copy(s, side):
        source, target = ((tokens, 0), (WINDOW, WINDOW + tokens))[side]
        step = (1, n_sp - 1)[side]
        return pltpu.make_async_remote_copy(
            src_ref=kv_buf.at[s, pl.ds(source, WINDOW), :],
            dst_ref=kv_buf.at[s, pl.ds(target, WINDOW), :],
            send_sem=ha_send.at[s, side],
            recv_sem=ha_recv.at[s, side],
            device_id={"sp": other(me_sp, step, n_sp)},
            device_id_type=MESH,
        )

    has_left, has_right = me_sp > 0, me_sp < n_sp - 1

    def halo_sends(s, act_on):
        for side, present in ((0, has_right), (1, has_left)):

            @pl.when(present)
            def _():
                act_on(halo_copy(s, side))

    def project(s, start):
        cols = slice(start, start + block)
        y = lax.dot_general(w_s[s], x_lat[s, cols, :], nt, preferred_element_type=f32)
        inv = inv_lat[s, :, cols]
        inv_q = inv * q_scale
        cr, sr = cos_row[:, cols], sin_row[:, cols]
        cc, sc = cos_col[...], sin_col[...]

        def wide(first, count):
            return jnp.concatenate([bias_col[s, first : first + count, :]] * (block // LANES), axis=1)

        def rotated(base, scale):
            u = [
                y[base + k * quarter : base + (k + 1) * quarter] * scale
                + wide(base + k * quarter, quarter)
                for k in range(4)
            ]
            return (
                u[0] * cr - u[1] * sr,
                u[0] * sr + u[1] * cr,
                u[2] * cc - u[3] * sc,
                u[2] * sc + u[3] * cc,
            )

        for h in range(heads):
            q_buf[s, h, 0:HEAD, cols] = jnp.concatenate(rotated(h * HEAD, inv_q), axis=0).astype(bf16)
        v = y[q_cols + HEAD :] * inv + wide(q_cols + HEAD, HEAD)
        kv = jnp.concatenate((*rotated(q_cols, inv), v), axis=0)
        vt_buf[s, 0:HEAD, WINDOW + start : WINDOW + start + block] = v.astype(bf16)
        kv_buf[s, WINDOW + start : WINDOW + start + block, :] = kv.T.astype(bf16)

    for s in range(samples):
        fold_sample(s)
        project(s, 0)
        project(s, tokens - block)
        halo_sends(s, lambda copy: copy.start())
        for i in range(1, n_tp - 1):
            project(s, i * block)
        if s > 0:
            context_keys(s)
            context_sends(s, first_turn)
        if s == 0:
            relay()

    halves = block // LANES

    to_across = 1 - 2 * lax.rem(me_tp, 2)
    to_along = 2 - 4 * lax.div(me_tp, 2)

    def partner(step):
        return me_tp + to_across * ((4 - step) // 2) + to_along * (step % 2)

    def rows_copy(s, step, source):
        target = partner(step)
        return pltpu.make_async_remote_copy(
            src_ref=att_buf.at[s, target],
            dst_ref=rows_rx.at[source, s],
            send_sem=at_send.at[s, step],
            recv_sem=at_recv.at[s, step],
            device_id={"tp": target},
            device_id_type=MESH,
        )

    pairs = heads // 2
    near_rows = LANES + 2 * WINDOW
    low = lax.broadcasted_iota(jnp.int32, (1, 2 * LANES), 1) < LANES

    def two(ref, pair):
        return jnp.where(low, ref[2 * pair], ref[2 * pair + 1]) * log2e

    def start_of(index):
        owner = partner(index // halves + 1)
        return pl.multiple_of(owner * block + (index % halves) * LANES, LANES)

    def chunks_of(near, far):
        return [(False, c, min(near, near_rows - c)) for c in range(0, near_rows, near)] + [
            (True, c, min(far, ctx_all)) for c in range(0, ctx_all, min(far, ctx_all))
        ]

    score_chunks = chunks_of(384, 256)
    value_chunks = chunks_of(256, 256)

    def score_steps(s, index, pair, buf, state):
        start = start_of(index)
        cols = pl.ds(start, LANES)
        q = jnp.concatenate(
            [q_buf[s, 2 * pair, :, cols], q_buf[s, 2 * pair + 1, :, cols]], axis=1
        )
        tops = [None, None]

        def one(chunk):
            far, first, count = chunk
            if far:
                keys = ckv_buf[s, first : first + count, :]
            else:
                keys = kv_buf[s, pl.ds(start + first, count), :]
            scores = jnp.dot(keys, q, preferred_element_type=f32)
            base = near_rows + first if far else first
            if not far:
                parts = [scores[r : r + WINDOW] for r in range(0, count, WINDOW)]
                for edge, place in ((0, 0), (1, near_rows - WINDOW)):
                    if first <= place < first + count:
                        mask = jnp.concatenate([mask_buf[edge], mask_buf[edge]], axis=1)
                        parts[(place - first) // WINDOW] += mask
                scores = jnp.concatenate(parts, axis=0)
            buf[base : base + count, :] = scores
            high = jnp.max(scores.reshape(count // 8, 8, 2 * LANES), axis=0)
            tops[far] = high if tops[far] is None else jnp.maximum(tops[far], high)

        for chunk in score_chunks:
            yield functools.partial(one, chunk)

        def close():
            near_top = jnp.max(tops[0], axis=0, keepdims=True)
            far_top = jnp.max(tops[1], axis=0, keepdims=True)
            lift = two(ctx_lift, pair)
            state.append(
                jnp.maximum(jnp.maximum(near_top, far_top + lift), two(sink_logit, pair))
            )

        yield close

    def value_steps(s, index, pair, buf, top):
        start = start_of(index)
        far_top = top - two(ctx_lift, pair)
        acc = [None]

        def one(chunk):
            far, first, count = chunk
            base = near_rows + first if far else first
            p = jnp.exp2(buf[base : base + count, :] - (far_top if far else top)).astype(bf16)
            if far:
                values = cvt_buf[s, :, first : first + count]
            else:
                values = vt_buf[s, :, pl.ds(start + first, count)]
            term = jnp.dot(values, p, preferred_element_type=f32)
            acc[0] = term if acc[0] is None else acc[0] + term

        for chunk in value_chunks:
            yield functools.partial(one, chunk)

        def close():
            weight = acc[0][HEAD : HEAD + 1] + jnp.exp2(two(sink_logit, pair) - top)
            rows = acc[0][0:HEAD] * (1.0 / weight)
            stacked = jnp.concatenate([rows[:, 0:LANES], rows[:, LANES:]], axis=0)
            owner = partner(index // halves + 1)
            half = pl.multiple_of((index % halves) * LANES, LANES)
            att_buf[s, owner, pl.ds(half, LANES), pair * LANES : (pair + 1) * LANES] = (
                stacked.T.astype(bf16)
            )

        yield close

    def run(*streams):
        streams = [list(steps) for steps in streams]
        order = sorted(
            ((i + 1) / len(steps), k, i) for k, steps in enumerate(streams) for i in range(len(steps))
        )
        for _, k, i in order:
            streams[k][i]()

    bufs = (s_a, s_b, s_c, s_d)
    per_step = halves * pairs

    def forward(kinds):
        for index in kinds:
            source = (across, along, diagonal)[index]
            for i in range(PIECES):
                if index == 2 or 2 * i // PIECES != index:
                    piece_arrive(index, i)
            for hop in range(1, n_dp):
                forward_copy(source, index, hop, me_dp).start()

    def attention(s):
        def scores_of(unit, base, target):
            return score_steps(s, base + unit // pairs, unit % pairs, bufs[unit % len(bufs)], target)

        tops = [[] for _ in range(AHEAD)]
        run(*(scores_of(unit, 0, tops[unit]) for unit in range(AHEAD)))

        def body(step, tops, last):
            base = step * halves
            known = [[top] for top in tops]
            for unit in range(per_step):
                streams = []
                if not last or unit + AHEAD < per_step:
                    known.append([])
                    streams.append(scores_of(unit + AHEAD, base, known[-1]))
                streams.append(
                    value_steps(
                        s, base + unit // pairs, unit % pairs, bufs[unit % len(bufs)], known[unit][0]
                    )
                )
                run(*streams)
            if not last:
                rows_copy(s, step + 1, me_tp).start()
                if s == samples - 1:
                    pl.when(step == 0)(lambda: forward((2,)))
            return tuple(top[0] for top in known[per_step:])

        tops = tuple(top[0] for top in tops)
        tops = lax.fori_loop(0, n_tp - 1, lambda step, tops: body(step, tops, False), tops)
        body(n_tp - 1, tops, True)
        rows_rx[me_tp, s] = att_buf[s, me_tp]

    def context_ready(s):
        for step in range(1, n_sp):
            ctx_copy(s, step, other(me_sp, n_sp - step, n_sp)).wait_recv()
        for c in range(0, ctx_all, 256):
            cvt_buf[s, 0:HEAD, c : c + 256] = ckv_buf[s, c : c + 256, :].T[HEAD:]

    def halo_ready(s):
        for side in range(2):
            first = (0, WINDOW + tokens)[side]
            valid = (has_left, has_right)[side]
            halo = slice(first, first + WINDOW)

            @pl.when(valid)
            def _():
                halo_copy(s, side).wait_recv()

            @pl.when(jnp.logical_not(valid))
            def _():
                kv_buf[s, halo, :] = jnp.zeros((WINDOW, LANES), bf16)
                vt_buf[s, HEAD:, halo] = jnp.zeros((ONES, WINDOW), bf16)

            vt_buf[s, 0:HEAD, halo] = kv_buf[s, halo, :].T[HEAD:]

    for s in range(samples):
        halo_ready(s)
        context_ready(s)
        if s + 1 < samples:
            context_sends(s + 1, jnp.logical_not(first_turn))
        attention(s)
        if s == 0:
            forward((0, 1))

    gate_b[1]()
    for t in range(n_tp):
        vec_g[0:keep_rows, t * part : (t + 1) * part] = gate_all[t]

    loads[-1].wait()
    for index, source in enumerate((across, along, diagonal)):
        for hop in range(1, n_dp):
            forward_copy(source, index, hop, other(me_dp, n_dp - hop, n_dp)).wait_recv()
    chunk = 512

    def rows_arrive(s, step):
        rows_copy(s, step, partner(step)).wait_recv()

    def mix(s, steps, c):
        acc = None
        for step in steps:
            t = partner(step) if step else me_tp
            term = jnp.dot(rows_rx[t, s], w_o[t, :, c : c + chunk], preferred_element_type=f32)
            acc = term if acc is None else acc + term
        return acc

    for s in range(samples):
        final = s == samples - 1
        for step in range(1, n_tp - 1 if final else n_tp):
            rows_arrive(s, step)
        for c in range(0, width, chunk):
            cols = slice(c, c + chunk)
            if final:
                mix_buf[:, cols] = mix(s, range(n_tp - 1), c)
            else:
                out[s, :, cols] = (mix(s, range(n_tp), c) * vec_g[s : s + 1, cols]).astype(bf16)
    rows_arrive(samples - 1, n_tp - 1)
    for c in range(0, width, chunk):
        cols = slice(c, c + chunk)
        acc = mix_buf[:, cols] + mix(samples - 1, (n_tp - 1,), c)
        out[samples - 1, :, cols] = (acc * vec_g[samples - 1 : samples, cols]).astype(bf16)

    for _, _, finish_send in (mod_a, mod_b, gate_a, gate_b):
        finish_send()
    for s in range(samples):
        for step in range(1, n_sp):
            ctx_copy(s, step, me_sp).wait_send()
        halo_sends(s, lambda copy: copy.wait_send())
    for i in range(PIECES):
        own_copy(0, i).wait_send()
        own_copy(1, i).wait_send()
        relay_copy(i).wait_send()
    for index, source in enumerate((across, along, diagonal)):
        for hop in range(1, n_dp):
            forward_copy(source, index, hop, me_dp).wait_send()
    for step in range(1, n_tp):
        for s in range(samples):
            rows_copy(s, step, me_tp).wait_send()


def fill_tables(first_row, cos_row, sin_row, cos_col, sin_col):
    tokens = cos_row.shape[1]
    quarter = HEAD // 4

    def pair(ticks, shape):
        power = lax.broadcasted_iota(jnp.int32, shape, 0).astype(f32)
        angles = ticks.astype(f32) * jnp.exp(power * (-math.log(rope_base) / quarter))
        return jnp.cos(angles), jnp.sin(angles)

    shape = cos_col.shape
    token = lax.broadcasted_iota(jnp.int32, shape, 1)
    cos_col[...], sin_col[...] = pair(token % GRID_COLS, shape)
    lines = tokens // GRID_COLS
    shape = (quarter, LANES)
    for first in range(0, lines, LANES):
        line = lax.broadcasted_iota(jnp.int32, shape, 1) + first + first_row
        cos_all, sin_all = pair(line, shape)
        half = lax.broadcasted_iota(jnp.int32, shape, 1) < GRID_COLS
        for r in range(0, min(LANES, lines - first), 2):
            cols = slice((first + r) * GRID_COLS, (first + r + 2) * GRID_COLS)
            for source, target in ((cos_all, cos_row), (sin_all, sin_row)):
                target[:, cols] = jnp.where(half, source[:, r : r + 1], source[:, r + 1 : r + 2])


def shards(
    latent,
    context,
    condition,
    ctx_cond,
    norm_gain,
    w_shift,
    w_scale,
    w_gate,
    w_query,
    w_key,
    w_value,
    w_out,
    sink_logit,
    ctx_lift,
):
    samples, tokens, width = latent.shape
    ctx_rows = context.shape[1]
    n_sp, n_tp, n_dp = lax.axis_size("sp"), lax.axis_size("tp"), lax.axis_size("dp")
    q_cols = w_query.shape[1]
    heads = q_cols // HEAD
    assert w_key.shape[1] == HEAD and tokens % GRID_COLS == 0 and samples < 4 and heads % 4 == 0 and n_tp == 4 and samples == 2
    part = w_shift.shape[1]
    block = tokens // n_tp
    ctx_all = n_sp * ctx_rows
    vmem = pl.BlockSpec(memory_space=pltpu.VMEM)
    anywhere = pl.BlockSpec(memory_space=pl.ANY)
    dma = pltpu.SemaphoreType.DMA
    padded = tokens + 2 * WINDOW
    proj = q_cols + 2 * HEAD
    keys = LANES + 2 * WINDOW + ctx_all
    V = pltpu.VMEM
    return pl.pallas_call(
        functools.partial(kernel, (n_sp, n_tp, n_dp)),
        out_shape=V((samples, block, width), bf16),
        in_specs=[anywhere] * 14,
        out_specs=vmem,
        scratch_shapes=[
            V(condition.shape, bf16),
            V(ctx_cond.shape, bf16),
            V((1, width), f32),
            pltpu.SMEM(sink_logit.shape, f32),
            pltpu.SMEM(ctx_lift.shape, f32),
            V(latent.shape, bf16),
            V(context.shape, bf16),
            V((3,) + w_shift.shape, bf16),
            V(w_query.shape, bf16),
            V((proj, width), bf16),
            V((samples, proj, width), bf16),
            V((2 * HEAD, width), bf16),
            V((HEAD // 4, tokens), f32),
            V((HEAD // 4, tokens), f32),
            V((HEAD // 4, block), f32),
            V((HEAD // 4, block), f32),
            V((n_tp,) + w_out.shape, bf16),
            V((8, w_shift.shape[0]), f32),
            V((n_sp, 4, 2 * part), bf16),
            V((n_tp, 4, 2 * part), bf16),
            V((n_sp, 4, part), f32),
            V((n_tp, 4, part), f32),
            V((8, width), f32),
            V((8, width), f32),
            V((8, width), f32),
            V((samples, 1, tokens), f32),
            V((samples, ctx_rows, LANES), f32),
            V((samples, proj, LANES), f32),
            V((8, 2 * HEAD), f32),
            V((samples, heads, LANES, tokens), bf16),
            V((samples, padded, LANES), bf16),
            V((samples, HEAD + ONES, padded), bf16),
            V((samples, ctx_all, LANES), bf16),
            V((samples, HEAD + ONES, ctx_all), bf16),
            V((2, WINDOW, LANES), f32),
            V((keys, 2 * LANES), f32),
            V((keys, 2 * LANES), f32),
            V((keys, 2 * LANES), f32),
            V((keys, 2 * LANES), f32),
            V((samples, n_tp, block, q_cols), bf16),
            V((n_tp, samples, block, q_cols), bf16),
            V((block, width), f32),
            dma((13 + samples,)),
            dma((n_sp,)),
            dma((n_sp,)),
            dma((n_tp,)),
            dma((n_tp,)),
            dma((n_sp,)),
            dma((n_sp,)),
            dma((n_tp,)),
            dma((n_tp,)),
            dma((samples, n_sp)),
            dma((samples, n_sp)),
            dma((samples, 2)),
            dma((samples, 2)),
            dma((samples, n_tp)),
            dma((samples, n_tp)),
            dma((3, PIECES)),
            dma((3, PIECES)),
            dma((3, n_dp)),
            dma((3, n_dp)),
        ],
        compiler_params=pltpu.CompilerParams(
            collective_id=0, has_side_effects=True, vmem_limit_bytes=56 * 1024 * 1024
        ),
    )(
        latent,
        context,
        condition,
        ctx_cond,
        norm_gain.reshape(1, -1),
        w_shift,
        w_scale,
        w_gate,
        w_query,
        w_key.T,
        w_value.T,
        w_out,
        sink_logit,
        ctx_lift,
    )


def solution(mesh):
    return jax.shard_map(
        shards,
        mesh=mesh,
        in_specs=(
            P("dp", "sp", None),
            P("dp", "sp", None),
            P("dp", "sp"),
            P("sp"),
            P(),
            P("sp", "tp"),
            P("sp", "tp"),
            P("sp", "tp"),
            P(None, "tp"),
            P(None, "tp"),
            P(None, "tp"),
            P("tp", None),
            P("tp"),
            P("tp"),
        ),
        out_specs=P("dp", ("sp", "tp"), None),
        check_vma=False,
    )
```
